256 devices in a mesh: grp: 2 (over y), sp: 32 (over z, core), tp: 4 (over x).
Axes of the slice: x: 4, y: 2, z: 16, core: 2. Of those that a mesh axis runs over, the one named last changes fastest.
The devices are a block of a 4x16x16 slice.
Arguments:
- query_plain: bfloat16 [10240, 1024], P(('grp', 'sp'), 'tp'), parts along dimension 0, may hold values from -6 to 6
- query_turn: bfloat16 [10240, 512], P(('grp', 'sp'), 'tp'), parts along dimension 0, may hold values from -40 to 40, as said below
- latent: bfloat16 [10240, 512], P(('grp', 'sp')), parts along dimension 0, may hold values from -6 to 6
- key_turn: bfloat16 [10240, 64], P(('grp', 'sp')), parts along dimension 0, may hold values from -40 to 40, as said below
- latent_norm_scale: bfloat16 [512], replicated, may hold values from 0.099609375 to 1.8984375
- plain_key_matrix: bfloat16 [512, 1024], P(None, 'tp'), may hold values from -0.25 to 0.25
- value_matrix: bfloat16 [512, 1024], P(None, 'tp'), may hold values from -0.25 to 0.25
- residual: bfloat16 [10240, 2048], P(('grp', 'sp', 'tp')), parts along dimension 0, may hold values from -6 to 6
- out_weight: bfloat16 [1024, 2048], replicated, may hold values from -6 to 6
- ffn_gain: bfloat16 [2048], replicated, may hold values from 0.099609375 to 1.8984375
- gate_weight: bfloat16 [32, 2048, 1024], P('sp', None, 'tp'), may hold values from -1 to 1
- up_weight: bfloat16 [32, 2048, 1024], P('sp', None, 'tp'), may hold values from -1 to 1
- down_weight: bfloat16 [32, 1024, 2048], P('sp', 'tp'), may hold values from -0.0625 to 0.0625
- routes: int32 [10240, 4], P(('grp', 'sp', 'tp')), parts along dimension 0, may hold values from 0 to 31, all different within a row; in each aligned block of 40 rows (0 to 39, 40 to 79, ...) at most 7 rows name the same one
- route_weights: float32 [10240, 4], P(('grp', 'sp', 'tp')), parts along dimension 0, may hold values from 0.1 to 0.6
Outputs:
- mixed: bfloat16 [10240, 2048], P(('grp', 'sp', 'tp')), parts along dimension 0
The draws below stay inside these ranges and needn't reach their ends.
There are 2 independent parts, one for each index of `grp`. The reference program is written for one: setup_inputs(seed, part) draws one part's arguments, and reference() takes and returns one part's arrays. A program takes and returns all parts, laid end to end along the dimension named above; an argument that names none is the same for every part. Nothing has to cross between parts.
Inputs may be any that keep to these rules, and one draw needn't show every extreme that they name: `query_turn`: in the hidden draw some rows are large. `key_turn`: in the hidden draw some rows are large. `routes`: each row names 4 different experts. In each aligned block of 40 rows (the rows of one device) no expert is named more than 7 times, a bound that some block reaches.
All inputs are finite; a program needn't handle non-finite values.
Results may differ from the reference program's by a relative error of at most 0.015.
Values may be sent and summed in bfloat16 or wider, within the bound.
A program may use at most 128 MiB of HBM per device.

```python
import math
import jax
import jax.numpy as jnp
import numpy as np
from jax import lax

D = 2048
ATTENTION_HEADS = 8
PLAIN_HEAD_WIDTH = 128
QK_ROPE = 64
VALUE_WIDTH = 128
LATENT_WIDTH = 512
D_EXPERT = 1024
TOP = 4
GRID_W = 64
ROWS_DEV = 40
SEQUENCE_TOKENS = 5120
EXPERTS = 32
CAP = 7
N_SP = 32
N_TP = 4


def draw_query_turn(key, part):
    base = jnp.clip(jax.random.normal(jax.random.fold_in(key, 1), (SEQUENCE_TOKENS, ATTENTION_HEADS * QK_ROPE), jnp.float32), -6.0, 6.0)
    return base.astype(jnp.bfloat16)


def draw_key_turn(key, part):
    base = jnp.clip(jax.random.normal(jax.random.fold_in(key, 2), (SEQUENCE_TOKENS, QK_ROPE), jnp.float32), -6.0, 6.0)
    return base.astype(jnp.bfloat16)


def block_scale(own_key, extent, cuts, least, high):
    loudness, own = 1.0, jax.random.fold_in(own_key, 6)
    for dim, shards_of in cuts:
        steps = jnp.exp(jax.random.uniform(jax.random.fold_in(own, dim), (shards_of,), jnp.float32, least / len(cuts), high / len(cuts)))
        loudness = loudness * jnp.repeat(steps, extent[dim] // shards_of).reshape([-1 if axis == dim else 1 for axis in range(len(extent))])
    return loudness


def shared_out(stream_key, own, number, rows, count, top, reach, skew):
    ranking = jax.random.permutation(stream_key, count)
    crowded, common = shares(count, rows * top, reach, skew, True), shares(count, rows * top, reach, skew, False)
    places = jnp.arange(count)

    def named(sizes, offset_by):
        used = int((sizes > 0).sum())
        fixed = max(1, used // 4)
        passed = fixed + (places - fixed + offset_by * (used - fixed)) % max(1, count - fixed)
        return jnp.zeros((count,), jnp.int32).at[ranking[jnp.where(places < fixed, places, passed)]].set(jnp.asarray(sizes, jnp.int32))

    sizes = jnp.where(number % 4 == 0, named(crowded, number // 4), named(common, number - number // 4 - 1))
    mixed = jax.random.permutation(jax.random.fold_in(own, 3), count)
    source_of, sink = mixed[0:count // 2 * 2:2], mixed[1:count // 2 * 2:2]
    slack = jnp.minimum(sizes[source_of] - 1, reach - sizes[sink]) // 2
    slack = jnp.where((source_of == ranking[0]) | (sink == ranking[0]) | (sizes[sink] == 0), 0, jnp.maximum(slack, 0))
    passed = jax.random.randint(jax.random.fold_in(own, 4), (count // 2,), 0, 1 << 20) % (slack + 1)
    sizes = sizes.at[source_of].add(-passed).at[sink].add(passed)
    members = jnp.searchsorted(jnp.cumsum(sizes), jnp.arange(rows * top), side="right").astype(jnp.int32)
    grid = members.reshape(top, rows).T
    grid = grid[jax.random.permutation(jax.random.fold_in(own, 1), rows)]
    offset_by = jax.random.randint(jax.random.fold_in(own, 2), (rows, 1), 0, top)
    return jnp.take_along_axis(grid, (jnp.arange(top)[None, :] + offset_by) % top, axis=1)


def shares(count, total, most, lean, full):
    loads = [(1 << 20) // math.isqrt(standing ** lean) + 1 for standing in range(1, count + 1)]
    largest = most if full else min(most, max(-(-total // count), total * loads[0] // sum(loads)))
    least = 1 if total - largest >= count - 1 else 0
    given, surplus = [largest] + [least] * (count - 1), total - largest - least * (count - 1)
    while surplus > 0:
        candidates = [i for i in range(1, count) if given[i] < largest] or [i for i in range(1, count) if given[i] < most]
        whole, budget = sum([loads[i] for i in candidates]), surplus
        for i in candidates:
            more = min(most - given[i], max(1, budget * loads[i] // whole), surplus)
            given[i] = given[i] + more
            surplus = surplus - more
    return np.array(given)


def scatter_about(own_key, dims, scale, bound, shards=(), kind=jnp.bfloat16):
    drawn = jax.random.normal(own_key, dims, jnp.float32) * scale
    if len(shards) > 0:
        drawn = block_scale(own_key, dims, shards, -0.22, 0.18) * drawn
    return jnp.clip(drawn, min=-bound, max=bound).astype(kind)


def setup_inputs(seed: int = 0, part: int = 0) -> dict:
    arg_keys = jax.random.split(jax.random.key(seed), 16)
    part_keys = jax.random.split(jax.random.fold_in(arg_keys[15], part), 16)
    query_plain = scatter_about(part_keys[0], (SEQUENCE_TOKENS, ATTENTION_HEADS * PLAIN_HEAD_WIDTH), 1.0, 6.0, ((0, 32), (1, 4)))
    query_turn = draw_query_turn(jax.random.fold_in(jax.random.fold_in(arg_keys[15], part), 71), part)
    latent = scatter_about(part_keys[2], (SEQUENCE_TOKENS, LATENT_WIDTH), 1.0, 6.0, ((0, 32),))
    key_turn = draw_key_turn(jax.random.fold_in(jax.random.fold_in(arg_keys[15], part), 71), part)
    latent_norm_scale = jnp.clip(1.0 + 0.18 * jax.random.normal(arg_keys[4], (LATENT_WIDTH,), jnp.float32), 0.099609375, 1.8984375).astype(jnp.bfloat16)
    plain_key_matrix = scatter_about(arg_keys[5], (LATENT_WIDTH, ATTENTION_HEADS * PLAIN_HEAD_WIDTH), LATENT_WIDTH ** -0.5, 0.25, ((1, 4),))
    value_matrix = scatter_about(arg_keys[6], (LATENT_WIDTH, ATTENTION_HEADS * VALUE_WIDTH), LATENT_WIDTH ** -0.5, 0.25, ((1, 4),))
    residual = scatter_about(part_keys[7], (SEQUENCE_TOKENS, D), 1.0, 6.0, ((0, 128),))
    out_weight = scatter_about(arg_keys[8], (ATTENTION_HEADS * VALUE_WIDTH, D), (16 * (ATTENTION_HEADS * VALUE_WIDTH) ** -0.5), 6.0)
    ffn_gain = jnp.clip(1.0 + 0.18 * jax.random.normal(arg_keys[9], (D,), jnp.float32), 0.099609375, 1.8984375).astype(jnp.bfloat16)
    gate_weight = scatter_about(arg_keys[10], (EXPERTS, D, D_EXPERT), (3 * D ** -0.5), 1.0, ((0, 32), (2, 4)))
    up_weight = scatter_about(arg_keys[11], (EXPERTS, D, D_EXPERT), (3 * D ** -0.5), 1.0, ((0, 32), (2, 4)))
    down_weight = scatter_about(arg_keys[12], (EXPERTS, D_EXPERT, D), (0.15 * D_EXPERT ** -0.5), 0.0625, ((0, 32), (1, 4)))
    routes_keys = jax.random.split(jax.random.fold_in(part_keys[13], 1), SEQUENCE_TOKENS // ROWS_DEV)
    routes_turns = jax.random.permutation(jax.random.fold_in(part_keys[13], 3), SEQUENCE_TOKENS // ROWS_DEV)
    routes = jax.vmap(lambda own, number: shared_out(jax.random.fold_in(part_keys[13], 2), own, number, ROWS_DEV, EXPERTS, TOP, CAP, 1))(routes_keys, routes_turns).reshape((SEQUENCE_TOKENS, TOP))
    route_weights = jnp.clip(0.1 + 0.5 * jax.random.uniform(part_keys[14], (SEQUENCE_TOKENS, TOP), jnp.float32) ** block_scale(part_keys[14], (SEQUENCE_TOKENS, TOP), ((0, 128),), -0.2, 0.2), 0.1, 0.6)
    return dict(query_plain=query_plain, query_turn=query_turn, latent=latent, key_turn=key_turn, latent_norm_scale=latent_norm_scale, plain_key_matrix=plain_key_matrix, value_matrix=value_matrix, residual=residual, out_weight=out_weight, ffn_gain=ffn_gain, gate_weight=gate_weight, up_weight=up_weight, down_weight=down_weight, routes=routes, route_weights=route_weights)


theta = 10000.0
eps = 1e-06
limit = 7.0
slope = 1.702

def turn(vector, row_shift, col_shift):
    width = vector.shape[-1]
    count = width // 4
    half = width // 2
    freqs = theta ** (-jnp.arange(count, dtype=jnp.float32) / count)
    extra = (1,) * (vector.ndim - 2)
    pieces = []
    for portion, shift in ((vector[..., :half], row_shift), (vector[..., half:], col_shift)):
        angle = (shift.astype(jnp.float32)[:, None] * freqs[None, :]).reshape((shift.shape[0],) + extra + (count,))
        lower = portion[..., :count]
        upper = portion[..., count:]
        pieces.append(jnp.concatenate([lower * jnp.cos(angle) - upper * jnp.sin(angle), lower * jnp.sin(angle) + upper * jnp.cos(angle)], axis=-1))
    return jnp.concatenate(pieces, axis=-1)

def norm_scale(values, gain):
    wide = values.astype(jnp.float32)
    return wide * lax.rsqrt(lax.optimization_barrier(jnp.mean(wide * wide, axis=-1, keepdims=True)) + eps) * gain.astype(jnp.float32)

def expert_apply(operands):
    rows, gate_w, up_w, down_w = operands
    gate_pre = jnp.minimum(jnp.dot(rows, gate_w, preferred_element_type=jnp.float32), limit)
    up_pre = jnp.clip(jnp.dot(rows, up_w, preferred_element_type=jnp.float32), -limit, limit)
    active = ((up_pre + 1.0) * gate_pre * jax.nn.sigmoid(slope * gate_pre)).astype(jnp.bfloat16)
    piece = down_w.shape[0] // N_TP
    groups = jnp.einsum('rnp,npd->nrd', active.reshape(rows.shape[0], N_TP, piece).astype(jnp.float32), down_w.reshape(N_TP, piece, down_w.shape[1]).astype(jnp.float32))
    rounded = lax.optimization_barrier(groups.astype(jnp.bfloat16))
    return lax.optimization_barrier(jnp.sum(rounded.astype(jnp.float32), axis=0)).astype(jnp.bfloat16)

def reference(query_plain, query_turn, latent, key_turn, latent_norm_scale, plain_key_matrix, value_matrix, residual, out_weight, ffn_gain, gate_weight, up_weight, down_weight, routes, route_weights):
    place = jnp.arange(SEQUENCE_TOKENS, dtype=jnp.int32)
    grid_row = place // GRID_W
    grid_col = place % GRID_W
    normed_latent = norm_scale(latent, latent_norm_scale).astype(jnp.bfloat16)
    key_plain = jnp.dot(normed_latent, plain_key_matrix, preferred_element_type=jnp.float32).astype(jnp.bfloat16)
    values = jnp.dot(normed_latent, value_matrix, preferred_element_type=jnp.float32).astype(jnp.bfloat16)
    key_rot = turn(key_turn.astype(jnp.float32), grid_row, grid_col).astype(jnp.bfloat16)
    query_rot = turn(query_turn.astype(jnp.float32).reshape(SEQUENCE_TOKENS, ATTENTION_HEADS, QK_ROPE), grid_row, grid_col).astype(jnp.bfloat16)
    plain_heads = jnp.moveaxis(query_plain.reshape(SEQUENCE_TOKENS, ATTENTION_HEADS, PLAIN_HEAD_WIDTH), 1, 0)
    rot_heads = jnp.moveaxis(query_rot, 1, 0)
    key_heads = jnp.moveaxis(key_plain.reshape(SEQUENCE_TOKENS, ATTENTION_HEADS, PLAIN_HEAD_WIDTH), 1, 0)
    value_heads = jnp.moveaxis(values.reshape(SEQUENCE_TOKENS, ATTENTION_HEADS, VALUE_WIDTH), 1, 0)
    scale = (PLAIN_HEAD_WIDTH + QK_ROPE) ** (-0.5)
    block = math.gcd(SEQUENCE_TOKENS, 512)

    def one_head(operands):
        head_plain, head_rot, head_keys, head_values = operands

        def one_block(start):
            block_plain = lax.dynamic_slice_in_dim(head_plain, start, block, 0)
            block_rot = lax.dynamic_slice_in_dim(head_rot, start, block, 0)
            scores = (jnp.einsum('qd,kd->qk', block_plain, head_keys, preferred_element_type=jnp.float32) + jnp.einsum('qd,kd->qk', block_rot, key_rot, preferred_element_type=jnp.float32)) * scale
            peak = lax.optimization_barrier(jnp.max(scores, axis=1, keepdims=True))
            weights = jnp.exp(scores - peak)
            summed = jnp.dot(weights.astype(jnp.bfloat16), head_values, preferred_element_type=jnp.float32)
            return (summed / lax.optimization_barrier(jnp.sum(weights, axis=1, keepdims=True))).astype(jnp.bfloat16)
        starts = jnp.arange(SEQUENCE_TOKENS // block, dtype=jnp.int32) * block
        return lax.map(one_block, starts).reshape(SEQUENCE_TOKENS, VALUE_WIDTH)
    attended = lax.map(one_head, (plain_heads, rot_heads, key_heads, value_heads))
    attended = jnp.moveaxis(attended, 0, 1).reshape(SEQUENCE_TOKENS, ATTENTION_HEADS * VALUE_WIDTH)
    hidden = (residual.astype(jnp.float32) + jnp.dot(attended, out_weight, preferred_element_type=jnp.float32)).astype(jnp.bfloat16)
    normed = norm_scale(hidden, ffn_gain).astype(jnp.bfloat16)
    blocks = N_SP * N_TP
    per_block = routes.reshape(blocks, ROWS_DEV * TOP)
    marks = (per_block[..., None] == jnp.arange(EXPERTS, dtype=jnp.int32)).astype(jnp.int32)
    earlier = jnp.cumsum(marks, axis=1, dtype=jnp.int32) - marks
    slots = lax.optimization_barrier(jnp.sum(earlier * marks, axis=2, dtype=jnp.int32))
    target = ((per_block * blocks + jnp.arange(blocks, dtype=jnp.int32)[:, None]) * CAP + slots).reshape(SEQUENCE_TOKENS * TOP)
    copies = jnp.repeat(normed, TOP, axis=0)
    buffer = jnp.zeros((EXPERTS * blocks * CAP, D), jnp.bfloat16).at[target].set(copies)
    results = lax.map(expert_apply, (buffer.reshape(EXPERTS, blocks * CAP, D), gate_weight, up_weight, down_weight))
    results = results.reshape(EXPERTS * blocks * CAP, D)
    picked = results[target].reshape(SEQUENCE_TOKENS, TOP, D).astype(jnp.float32)
    return (hidden.astype(jnp.float32) + lax.optimization_barrier(jnp.sum(route_weights[..., None] * picked, axis=1))).astype(jnp.bfloat16)
```

```python
import functools

import jax
import jax.numpy as jnp
from jax import lax
from jax.experimental import pallas as pl
from jax.experimental.pallas import tpu as pltpu
from jax.sharding import Mesh
from jax.sharding import PartitionSpec as P

PLAIN_HEAD_WIDTH = 128
QK_ROPE = 64
VALUE_WIDTH = 128
GRID_W = 64
SP = ("sp_0", "sp_1")
GRP_SP = ("grp", "sp_0", "sp_1")
GRP_SP_TP = ("grp", "sp_0", "sp_1", "tp")
MESH = pl.DeviceIdType.MESH

theta = 10000.0
eps = 1e-06
limit = 7.0
slope = 1.702

SLOTS = 8
HALF = 64
SPLIT = 2


def sent_together(arrays, axis, dim, along):
    both = jnp.concatenate(arrays, axis=along)
    result, at, finished = (lax.all_gather(both, axis, axis=dim, tiled=True), 0, [])
    for a in arrays:
        finished.append(lax.slice_in_dim(result, at, at + a.shape[along], axis=along))
        at += a.shape[along]
    return tuple(finished)


def turn(vector, row_shift, col_shift):
    width = vector.shape[-1]
    count = width // 4
    half = width // 2
    freqs = theta ** (-jnp.arange(count, dtype=jnp.float32) / count)
    extra = (1,) * (vector.ndim - 2)
    pieces = []
    for portion, shift in ((vector[..., :half], row_shift), (vector[..., half:], col_shift)):
        angle = (shift.astype(jnp.float32)[:, None] * freqs[None, :]).reshape(
            (shift.shape[0],) + extra + (count,)
        )
        lower = portion[..., :count]
        upper = portion[..., count:]
        pieces.append(
            jnp.concatenate(
                [
                    lower * jnp.cos(angle) - upper * jnp.sin(angle),
                    lower * jnp.sin(angle) + upper * jnp.cos(angle),
                ],
                axis=-1,
            )
        )
    return jnp.concatenate(pieces, axis=-1)


def norm_scale(values, gain):
    wide = values.astype(jnp.float32)
    return (
        wide
        * lax.rsqrt(jnp.mean(wide * wide, axis=-1, keepdims=True) + eps)
        * gain.astype(jnp.float32)
    )


def greet(peers):
    barrier = pltpu.get_barrier_semaphore()
    for peer in peers:
        pl.semaphore_signal(barrier, inc=1, device_id=peer, device_id_type=MESH)
    pl.semaphore_wait(barrier, len(peers))


def places():
    z = lax.axis_index("sp_0")
    c = lax.axis_index("sp_1")
    x = lax.axis_index("tp")
    count = lax.axis_size("sp_0")
    after = lax.rem(z + 1, count)
    before = lax.rem(z + count - 1, count)
    mirror = lax.axis_size("tp") - 1 - x
    ring = ({"sp_0": after}, {"sp_0": before})
    near = ({"sp_1": 1 - c}, {"tp": mirror}, {"sp_1": 1 - c, "tp": mirror})
    return z, c, ring, near


def matches(z, c, merged):
    row = lax.broadcasted_iota(jnp.int32, (4 * SLOTS, 2 * HALF), 0)
    lane = lax.broadcasted_iota(jnp.int32, (4 * SLOTS, 2 * HALF), 1)
    core = jnp.where(row < 2 * SLOTS, c, 1 - c)
    wanted = ((2 * z + core) * SLOTS + row % SLOTS).astype(jnp.float32)
    same = (row // SLOTS) % 2 == lane // HALF
    return [
        jnp.logical_and(same, jnp.broadcast_to(merged[k : k + 1], wanted.shape) == wanted)
        for k in range(4)
    ]


def merged_notes(first, second):
    return jnp.concatenate(
        [first[...].astype(jnp.float32)[:, :HALF], second[...].astype(jnp.float32)[:, :HALF]],
        axis=1,
    )


def dispatch_kernel(
    norm_ref,
    note_ref,
    sent_ref,
    notes_ref,
    blocks,
    notes,
    chosen,
    ring_send,
    ring_recv,
    note_send,
    note_recv,
    near_send,
    near_recv,
    own_sem,
):
    z, c, ring, near = places()
    steps, _, width = blocks.shape
    rows = norm_ref.shape[0]
    part = width // SPLIT
    last = (steps - 1, steps - 2)
    for j in range(steps):
        for d in range(2):
            blocks[j, d * HALF + rows : (d + 1) * HALF] = jnp.zeros(
                (HALF - rows, width), blocks.dtype
            )
    greet((*ring, *near))

    def ring_copy(d, j, h):
        columns = pl.ds(h * part, part)
        span = pl.ds(d * HALF, rows)
        source = norm_ref.at[:, columns] if j == 0 else blocks.at[j - 1, span, columns]
        return pltpu.make_async_remote_copy(
            src_ref=source,
            dst_ref=blocks.at[j, span, columns],
            send_sem=ring_send.at[d, j, h],
            recv_sem=ring_recv.at[d, j, h],
            device_id=ring[d],
            device_id_type=MESH,
        )

    def note_copy(d, j):
        return pltpu.make_async_remote_copy(
            src_ref=note_ref if j == 0 else notes.at[d, j - 1],
            dst_ref=notes.at[d, j],
            send_sem=note_send.at[d, j],
            recv_sem=note_recv.at[d, j],
            device_id=ring[d],
            device_id_type=MESH,
        )

    def near_copy(j, q):
        return pltpu.make_async_remote_copy(
            src_ref=chosen.at[j, pl.ds((q % 2) * 2 * SLOTS, 2 * SLOTS)],
            dst_ref=sent_ref.at[j, pl.ds(q * 2 * SLOTS, 2 * SLOTS)],
            send_sem=near_send.at[j, q - 1],
            recv_sem=near_recv.at[j, q - 1],
            device_id=near[q - 1],
            device_id_type=MESH,
        )

    def own_copy(j):
        return pltpu.make_async_copy(
            chosen.at[j, pl.ds(0, 2 * SLOTS)], sent_ref.at[j, pl.ds(0, 2 * SLOTS)], own_sem.at[j]
        )

    for d in range(2):
        note_copy(d, 0).start()
    for h in range(SPLIT):
        for d in range(2):
            ring_copy(d, 0, h).start()
    blocks[steps - 1, HALF : HALF + rows] = norm_ref[...]
    notes[1, steps - 1] = note_ref[...]
    for j in range(steps):
        for d in range(2):
            if j <= last[d]:
                note_copy(d, j).wait_recv()
                if j < last[d]:
                    note_copy(d, j + 1).start()
        for h in range(SPLIT):
            for d in range(2):
                if j <= last[d]:
                    ring_copy(d, j, h).wait_recv()
                    if j < last[d]:
                        ring_copy(d, j + 1, h).start()
        merged = merged_notes(notes.at[0, j], notes.at[1, j])
        notes_ref[j] = merged
        found = matches(z, c, merged)
        picks = sum(m.astype(jnp.float32) for m in found).astype(jnp.bfloat16)
        chosen[j] = jnp.dot(picks, blocks[j], preferred_element_type=jnp.float32).astype(
            jnp.bfloat16
        )
        own_copy(j).start()
        for q in (2, 3, 1):
            near_copy(j, q).start()
    for j in range(steps):
        for d in range(2):
            if j <= last[d]:
                note_copy(d, j).wait_send()
                for h in range(SPLIT):
                    ring_copy(d, j, h).wait_send()
        own_copy(j).wait()
        for q in (1, 2, 3):
            near_copy(j, q).wait()


def dispatch(normed, note, steps):
    rows, width = normed.shape
    return pl.pallas_call(
        dispatch_kernel,
        name="dispatch",
        out_shape=(
            jax.ShapeDtypeStruct((steps, 8 * SLOTS, width), jnp.bfloat16),
            jax.ShapeDtypeStruct((steps, 16, 2 * HALF), jnp.float32),
        ),
        in_specs=[pl.BlockSpec(memory_space=pltpu.VMEM)] * 2,
        out_specs=(
            pl.BlockSpec(memory_space=pl.ANY),
            pl.BlockSpec(memory_space=pltpu.VMEM),
        ),
        scratch_shapes=[
            pltpu.VMEM((steps, 2 * HALF, width), jnp.bfloat16),
            pltpu.VMEM((2, steps, 16, 2 * HALF), jnp.bfloat16),
            pltpu.VMEM((steps, 4 * SLOTS, width), jnp.bfloat16),
            pltpu.SemaphoreType.DMA((2, steps, SPLIT)),
            pltpu.SemaphoreType.DMA((2, steps, SPLIT)),
            pltpu.SemaphoreType.DMA((2, steps)),
            pltpu.SemaphoreType.DMA((2, steps)),
            pltpu.SemaphoreType.DMA((steps, 3)),
            pltpu.SemaphoreType.DMA((steps, 3)),
            pltpu.SemaphoreType.DMA((steps,)),
        ],
        compiler_params=pltpu.CompilerParams(
            collective_id=1, has_side_effects=True, vmem_limit_bytes=40 * 2**20
        ),
        cost_estimate=pl.CostEstimate(
            flops=30_000_000_000, bytes_accessed=8_000_000, transcendentals=0
        ),
    )(normed, note)


def combine_kernel(
    sent_ref,
    notes_ref,
    gate_ref,
    up_ref,
    down_ref,
    gate2_ref,
    up2_ref,
    down2_ref,
    out_ref,
    taken,
    gate_w,
    up_w,
    down_w,
    product,
    back,
    token,
    own,
    arrive,
    leave,
    load_sem,
    weight_sem,
    near_send,
    near_recv,
    ring_send,
    ring_recv,
):
    z, c, ring, near = places()
    steps, taken_rows, width = taken.shape
    rows = out_ref.shape[0]
    part = width // SPLIT
    span = 2 * SLOTS
    group = steps // 2
    halves = ((group, steps), (0, group))
    loads = [
        pltpu.make_async_copy(
            sent_ref.at[pl.ds(a, b - a)], taken.at[pl.ds(a, b - a)], load_sem.at[i]
        )
        for i, (a, b) in enumerate(halves)
    ]
    weights = [
        pltpu.make_async_copy(source, target.at[i // 3], weight_sem.at[i])
        for i, (source, target) in enumerate(
            (
                (gate_ref, gate_w),
                (up_ref, up_w),
                (down_ref, down_w),
                (gate2_ref, gate_w),
                (up2_ref, up_w),
                (down2_ref, down_w),
            )
        )
    ]
    loads[0].start()
    for w in weights[:2]:
        w.start()
    loads[1].start()
    for w in weights[2:]:
        w.start()
    greet((*ring, *near))

    def near_copy(j, q):
        return pltpu.make_async_remote_copy(
            src_ref=product.at[j, pl.ds(q * span, span)],
            dst_ref=back.at[j, pl.ds(q * span, span)],
            send_sem=near_send.at[j, q - 1],
            recv_sem=near_recv.at[j, q - 1],
            device_id=near[q - 1],
            device_id_type=MESH,
        )

    def ring_copy(d, j, h):
        columns = pl.ds(h * part, part)
        slot = j - 1 if j > 0 else steps - 1
        return pltpu.make_async_remote_copy(
            src_ref=leave.at[d, j, :, columns],
            dst_ref=arrive.at[d, slot, :, columns],
            send_sem=ring_send.at[d, j, h],
            recv_sem=ring_recv.at[d, j, h],
            device_id=ring[1 - d],
            device_id_type=MESH,
        )

    for i, (a, b) in enumerate(halves):
        loads[i].wait()
        x = taken[a:b].reshape((b - a) * taken_rows, width)
        result = None
        for half in range(2):
            if i == 0:
                weights[3 * half].wait()
            gate = jnp.minimum(
                jnp.dot(x, gate_w[half], preferred_element_type=jnp.float32), limit
            )
            if i == 0:
                weights[3 * half + 1].wait()
            up = jnp.clip(
                jnp.dot(x, up_w[half], preferred_element_type=jnp.float32), -limit, limit
            )
            active = ((up + 1.0) * gate * jax.nn.sigmoid(slope * gate)).astype(jnp.bfloat16)
            if i == 0:
                weights[3 * half + 2].wait()
            term = jnp.dot(active, down_w[half], preferred_element_type=jnp.float32)
            result = term if result is None else result + term
        product[a:b] = result.astype(jnp.bfloat16).reshape(b - a, taken_rows, width)
        for j in range(b - 1, a - 1, -1):
            for q in (2, 3, 1):
                near_copy(j, q).start()
            back[j, 0:span] = product[j, 0:span]

    first = (steps - 1, steps - 2)
    for j in range(steps - 1, -1, -1):
        merged = notes_ref[j]
        found = matches(z, c, merged)
        tables = []
        for base in (4, 8):
            table = sum(
                jnp.where(m, jnp.broadcast_to(merged[base + k : base + k + 1], m.shape), 0.0)
                for k, m in enumerate(found)
            )
            flat = jnp.transpose(table)
            tables.append(jnp.concatenate([flat, flat], axis=1).astype(jnp.bfloat16))
        for q in (1, 2, 3):
            near_copy(j, q).wait_recv()
        token[...] = jnp.dot(tables[0], back[j], preferred_element_type=jnp.float32) + jnp.dot(
            tables[1], back[j], preferred_element_type=jnp.float32
        )
        if j == steps - 1:
            own[...] = token[HALF : HALF + rows]
        for h in range(SPLIT):
            columns = slice(h * part, (h + 1) * part)
            for d in range(2):
                if j > first[d]:
                    continue
                total = token[d * HALF : d * HALF + rows, columns]
                if j < first[d]:
                    ring_copy(d, j + 1, h).wait_recv()
                    total = total + arrive[d, j, :, columns].astype(jnp.float32)
                leave[d, j, :, columns] = total.astype(jnp.bfloat16)
                ring_copy(d, j, h).start()
    for h in range(SPLIT):
        columns = slice(h * part, (h + 1) * part)
        for d in range(2):
            ring_copy(d, 0, h).wait_recv()
        out_ref[:, columns] = (
            own[:, columns]
            + arrive[0, steps - 1, :, columns].astype(jnp.float32)
            + arrive[1, steps - 1, :, columns].astype(jnp.float32)
        )
    for j in range(steps):
        for q in (1, 2, 3):
            near_copy(j, q).wait_send()
        for d in range(2):
            if j <= first[d]:
                for h in range(SPLIT):
                    ring_copy(d, j, h).wait_send()


def combine(sent, notes, weights, rows):
    steps, taken_rows, width = sent.shape
    hidden_units = weights[0].shape[1]
    any_space = pl.BlockSpec(memory_space=pl.ANY)
    vmem = pl.BlockSpec(memory_space=pltpu.VMEM)
    bf16 = jnp.bfloat16
    return pl.pallas_call(
        combine_kernel,
        name="combine",
        out_shape=jax.ShapeDtypeStruct((rows, width), jnp.float32),
        in_specs=[any_space, vmem] + [any_space] * 6,
        out_specs=vmem,
        scratch_shapes=[
            pltpu.VMEM((steps, taken_rows, width), bf16),
            pltpu.VMEM((2, width, hidden_units), bf16),
            pltpu.VMEM((2, width, hidden_units), bf16),
            pltpu.VMEM((2, hidden_units, width), bf16),
            pltpu.VMEM((steps, taken_rows, width), bf16),
            pltpu.VMEM((steps, taken_rows, width), bf16),
            pltpu.VMEM((2 * HALF, width), jnp.float32),
            pltpu.VMEM((rows, width), jnp.float32),
            pltpu.VMEM((2, steps, rows, width), bf16),
            pltpu.VMEM((2, steps, rows, width), bf16),
            pltpu.SemaphoreType.DMA((2,)),
            pltpu.SemaphoreType.DMA((6,)),
            pltpu.SemaphoreType.DMA((steps, 3)),
            pltpu.SemaphoreType.DMA((steps, 3)),
            pltpu.SemaphoreType.DMA((2, steps, SPLIT)),
            pltpu.SemaphoreType.DMA((2, steps, SPLIT)),
        ],
        compiler_params=pltpu.CompilerParams(
            collective_id=2, has_side_effects=True, vmem_limit_bytes=56 * 2**20
        ),
        cost_estimate=pl.CostEstimate(
            flops=30_000_000_000, bytes_accessed=8_000_000, transcendentals=0
        ),
    )(sent, notes, *weights)


def routing_note(routes, route_weights, experts):
    rows, top = routes.shape
    flat = routes.reshape(rows * top)
    marks = (flat[:, None] == jnp.arange(experts, dtype=jnp.int32)[None, :]).astype(jnp.int32)
    earlier = jnp.cumsum(marks, axis=0, dtype=jnp.int32) - marks
    slots = jnp.sum(earlier * marks, axis=1, dtype=jnp.int32)
    target = (flat * SLOTS + slots).reshape(rows, top)
    high = route_weights.astype(jnp.bfloat16)
    low = (route_weights - high.astype(jnp.float32)).astype(jnp.bfloat16)
    parts = jnp.concatenate([target.astype(jnp.bfloat16), high, low], axis=1).T
    return jnp.pad(
        parts, ((0, 16 - 3 * top), (0, 2 * HALF - rows)), constant_values=-1.0
    )


def on_device(
    query_plain,
    query_turn,
    latent,
    key_turn,
    latent_norm_scale,
    plain_key_matrix,
    value_matrix,
    residual,
    out_weight,
    ffn_gain,
    gate_weight,
    up_weight,
    down_weight,
    routes,
    route_weights,
):
    tok_dev = latent.shape[0]
    heads_dev = query_plain.shape[1] // PLAIN_HEAD_WIDTH
    tp = lax.axis_size("tp")
    swap = [(i, i ^ 1) for i in range(tp)]
    own_weights = (gate_weight[0], up_weight[0], down_weight[0])
    other_weights = tuple(lax.ppermute(w, "tp", swap) for w in own_weights)
    experts_all = lax.axis_size(SP) * gate_weight.shape[0]
    note = routing_note(routes, route_weights, experts_all)
    place = lax.axis_index(SP) * tok_dev + jnp.arange(tok_dev, dtype=jnp.int32)
    grid_row = place // GRID_W
    grid_col = place % GRID_W
    normed_latent = norm_scale(latent, latent_norm_scale).astype(jnp.bfloat16)
    key_plain = jnp.dot(normed_latent, plain_key_matrix, preferred_element_type=jnp.float32).astype(
        jnp.bfloat16
    )
    values = jnp.dot(normed_latent, value_matrix, preferred_element_type=jnp.float32).astype(
        jnp.bfloat16
    )
    key_rot = turn(key_turn.astype(jnp.float32), grid_row, grid_col).astype(jnp.bfloat16)
    key_pairs = key_rot.reshape(tok_dev // 2, 2 * QK_ROPE)
    query_rot = turn(
        query_turn.astype(jnp.float32).reshape(tok_dev, heads_dev, QK_ROPE), grid_row, grid_col
    ).astype(jnp.bfloat16)
    plain_query = query_plain.reshape(tok_dev, heads_dev, PLAIN_HEAD_WIDTH)
    scale = (PLAIN_HEAD_WIDTH + QK_ROPE) ** (-0.5)
    piece_keys, piece_values, piece_pairs = (
        *sent_together((key_plain, values), SP, 0, 1),
        lax.all_gather(key_pairs, SP, axis=0, tiled=True),
    )
    count = piece_keys.shape[0]
    piece_rot = piece_pairs.reshape(count, QK_ROPE)
    new_total = []
    new_summed = []
    for head in range(heads_dev):
        head_keys = piece_keys[:, head * PLAIN_HEAD_WIDTH : (head + 1) * PLAIN_HEAD_WIDTH]
        head_values = piece_values[:, head * VALUE_WIDTH : (head + 1) * VALUE_WIDTH]
        scores = (
            jnp.einsum(
                "qd,kd->qk", plain_query[:, head], head_keys, preferred_element_type=jnp.float32
            )
            + jnp.einsum(
                "qd,kd->qk", query_rot[:, head], piece_rot, preferred_element_type=jnp.float32
            )
        ) * scale
        peak = jnp.max(scores, axis=1)
        weights = jnp.exp(scores - peak[:, None])
        new_total.append(jnp.sum(weights, axis=1))
        new_summed.append(
            jnp.dot(weights.astype(jnp.bfloat16), head_values, preferred_element_type=jnp.float32)
        )
    total = jnp.stack(new_total)
    summed = jnp.stack(new_summed)
    attended = jnp.transpose((summed / total[..., None]).astype(jnp.bfloat16), (1, 0, 2)).reshape(
        tok_dev, heads_dev * VALUE_WIDTH
    )
    rows_dev = residual.shape[0]
    token_heads = lax.all_to_all(attended, "tp", split_axis=0, concat_axis=1, tiled=True)
    projected = jnp.dot(token_heads, out_weight, preferred_element_type=jnp.float32)
    hidden = (residual.astype(jnp.float32) + projected).astype(jnp.bfloat16)
    normed = norm_scale(hidden, ffn_gain).astype(jnp.bfloat16)
    sent, notes = dispatch(normed, note, lax.axis_size("sp_0") // 2)
    mixed = combine(sent, notes, (*own_weights, *other_weights), rows_dev)
    return (hidden.astype(jnp.float32) + mixed).astype(jnp.bfloat16)


def solution(mesh):
    torus = Mesh(
        mesh.devices.reshape(mesh.shape["grp"], mesh.shape["sp"] // 2, 2, mesh.shape["tp"]),
        ("grp", "sp_0", "sp_1", "tp"),
    )
    placed = (
        P(GRP_SP, "tp"),
        P(GRP_SP, "tp"),
        P(GRP_SP, None),
        P(GRP_SP, None),
        P(),
        P(None, "tp"),
        P(None, "tp"),
        P(GRP_SP_TP, None),
        P(),
        P(),
        P(SP, None, "tp"),
        P(SP, None, "tp"),
        P(SP, "tp", None),
        P(GRP_SP_TP, None),
        P(GRP_SP_TP, None),
    )
    return jax.shard_map(
        on_device, mesh=torus, in_specs=placed, out_specs=P(GRP_SP_TP, None), check_vma=False
    )
```

```python
import functools

import jax
import jax.numpy as jnp
from jax import lax
from jax.experimental import pallas as pl
from jax.experimental.pallas import tpu as pltpu
from jax.sharding import Mesh
from jax.sharding import PartitionSpec as P

PLAIN_HEAD_WIDTH = 128
QK_ROPE = 64
VALUE_WIDTH = 128
GRID_W = 64
SP = ("sp_0", "sp_1")
GRP_SP = ("grp", "sp_0", "sp_1")
GRP_SP_TP = ("grp", "sp_0", "sp_1", "tp")
MESH = pl.DeviceIdType.MESH

theta = 10000.0
eps = 1e-06
limit = 7.0
slope = 1.702

SLOTS = 8
HALF = 64
SPLIT = 2


def turn(vector, row_shift, col_shift):
    width = vector.shape[-1]
    count = width // 4
    half = width // 2
    freqs = theta ** (-jnp.arange(count, dtype=jnp.float32) / count)
    extra = (1,) * (vector.ndim - 2)
    pieces = []
    for portion, shift in ((vector[..., :half], row_shift), (vector[..., half:], col_shift)):
        angle = (shift.astype(jnp.float32)[:, None] * freqs[None, :]).reshape(
            (shift.shape[0],) + extra + (count,)
        )
        lower = portion[..., :count]
        upper = portion[..., count:]
        pieces.append(
            jnp.concatenate(
                [
                    lower * jnp.cos(angle) - upper * jnp.sin(angle),
                    lower * jnp.sin(angle) + upper * jnp.cos(angle),
                ],
                axis=-1,
            )
        )
    return jnp.concatenate(pieces, axis=-1)


def greet(peers):
    barrier = pltpu.get_barrier_semaphore()
    for peer in peers:
        pl.semaphore_signal(barrier, inc=1, device_id=peer, device_id_type=MESH)
    pl.semaphore_wait(barrier, len(peers))


def places():
    z = lax.axis_index("sp_0")
    c = lax.axis_index("sp_1")
    x = lax.axis_index("tp")
    count = lax.axis_size("sp_0")
    after = lax.rem(z + 1, count)
    before = lax.rem(z + count - 1, count)
    mirror = lax.axis_size("tp") - 1 - x
    ring = ({"sp_0": after}, {"sp_0": before})
    near = ({"sp_1": 1 - c}, {"tp": mirror}, {"sp_1": 1 - c, "tp": mirror})
    return z, c, ring, near


def matches(z, c, merged):
    row = lax.broadcasted_iota(jnp.int32, (4 * SLOTS, 2 * HALF), 0)
    lane = lax.broadcasted_iota(jnp.int32, (4 * SLOTS, 2 * HALF), 1)
    core = jnp.where(row < 2 * SLOTS, c, 1 - c)
    wanted = ((2 * z + core) * SLOTS + row % SLOTS).astype(jnp.float32)
    same = (row // SLOTS) % 2 == lane // HALF
    return [
        jnp.logical_and(same, jnp.broadcast_to(merged[k : k + 1], wanted.shape) == wanted)
        for k in range(4)
    ]


def merged_notes(first, second):
    return jnp.concatenate(
        [first[...].astype(jnp.float32)[:, :HALF], second[...].astype(jnp.float32)[:, :HALF]],
        axis=1,
    )


def dispatch_kernel(
    norm_ref,
    note_ref,
    sent_ref,
    notes_ref,
    blocks,
    notes,
    chosen,
    ring_send,
    ring_recv,
    note_send,
    note_recv,
    near_send,
    near_recv,
    own_sem,
):
    z, c, ring, near = places()
    steps, _, width = blocks.shape
    rows = norm_ref.shape[0]
    part = width // SPLIT
    last = (steps - 1, steps - 2)
    for j in range(steps):
        for d in range(2):
            blocks[j, d * HALF + rows : (d + 1) * HALF] = jnp.zeros(
                (HALF - rows, width), blocks.dtype
            )
    greet((*ring, *near))

    def ring_copy(d, j, h):
        columns = pl.ds(h * part, part)
        span = pl.ds(d * HALF, rows)
        source = norm_ref.at[:, columns] if j == 0 else blocks.at[j - 1, span, columns]
        return pltpu.make_async_remote_copy(
            src_ref=source,
            dst_ref=blocks.at[j, span, columns],
            send_sem=ring_send.at[d, j, h],
            recv_sem=ring_recv.at[d, j, h],
            device_id=ring[d],
            device_id_type=MESH,
        )

    def note_copy(d, j):
        return pltpu.make_async_remote_copy(
            src_ref=note_ref if j == 0 else notes.at[d, j - 1],
            dst_ref=notes.at[d, j],
            send_sem=note_send.at[d, j],
            recv_sem=note_recv.at[d, j],
            device_id=ring[d],
            device_id_type=MESH,
        )

    def near_copy(j, q):
        return pltpu.make_async_remote_copy(
            src_ref=chosen.at[j, pl.ds((q % 2) * 2 * SLOTS, 2 * SLOTS)],
            dst_ref=sent_ref.at[j, pl.ds(q * 2 * SLOTS, 2 * SLOTS)],
            send_sem=near_send.at[j, q - 1],
            recv_sem=near_recv.at[j, q - 1],
            device_id=near[q - 1],
            device_id_type=MESH,
        )

    def own_copy(j):
        return pltpu.make_async_copy(
            chosen.at[j, pl.ds(0, 2 * SLOTS)], sent_ref.at[j, pl.ds(0, 2 * SLOTS)], own_sem.at[j]
        )

    for d in range(2):
        note_copy(d, 0).start()
    for h in range(SPLIT):
        for d in range(2):
            ring_copy(d, 0, h).start()
    blocks[steps - 1, HALF : HALF + rows] = norm_ref[...]
    notes[1, steps - 1] = note_ref[...]
    for j in range(steps):
        for d in range(2):
            if j <= last[d]:
                note_copy(d, j).wait_recv()
                if j < last[d]:
                    note_copy(d, j + 1).start()
        for h in range(SPLIT):
            for d in range(2):
                if j <= last[d]:
                    ring_copy(d, j, h).wait_recv()
                    if j < last[d]:
                        ring_copy(d, j + 1, h).start()
        merged = merged_notes(notes.at[0, j], notes.at[1, j])
        notes_ref[j] = merged
        found = matches(z, c, merged)
        picks = sum(m.astype(jnp.float32) for m in found).astype(jnp.bfloat16)
        chosen[j] = jnp.dot(picks, blocks[j], preferred_element_type=jnp.float32).astype(
            jnp.bfloat16
        )
        own_copy(j).start()
        for q in (2, 3, 1):
            near_copy(j, q).start()
    for j in range(steps):
        for d in range(2):
            if j <= last[d]:
                note_copy(d, j).wait_send()
                for h in range(SPLIT):
                    ring_copy(d, j, h).wait_send()
        own_copy(j).wait()
        for q in (1, 2, 3):
            near_copy(j, q).wait()


def dispatch(normed, note, steps):
    rows, width = normed.shape
    return pl.pallas_call(
        dispatch_kernel,
        name="dispatch",
        out_shape=(
            jax.ShapeDtypeStruct((steps, 8 * SLOTS, width), jnp.bfloat16),
            jax.ShapeDtypeStruct((steps, 16, 2 * HALF), jnp.float32),
        ),
        in_specs=[pl.BlockSpec(memory_space=pltpu.VMEM)] * 2,
        out_specs=(
            pl.BlockSpec(memory_space=pl.ANY),
            pl.BlockSpec(memory_space=pltpu.VMEM),
        ),
        scratch_shapes=[
            pltpu.VMEM((steps, 2 * HALF, width), jnp.bfloat16),
            pltpu.VMEM((2, steps, 16, 2 * HALF), jnp.bfloat16),
            pltpu.VMEM((steps, 4 * SLOTS, width), jnp.bfloat16),
            pltpu.SemaphoreType.DMA((2, steps, SPLIT)),
            pltpu.SemaphoreType.DMA((2, steps, SPLIT)),
            pltpu.SemaphoreType.DMA((2, steps)),
            pltpu.SemaphoreType.DMA((2, steps)),
            pltpu.SemaphoreType.DMA((steps, 3)),
            pltpu.SemaphoreType.DMA((steps, 3)),
            pltpu.SemaphoreType.DMA((steps,)),
        ],
        compiler_params=pltpu.CompilerParams(
            collective_id=1, has_side_effects=True, vmem_limit_bytes=40 * 2**20
        ),
        cost_estimate=pl.CostEstimate(
            flops=30_000_000_000, bytes_accessed=8_000_000, transcendentals=0
        ),
    )(normed, note)


def combine_kernel(
    sent_ref,
    notes_ref,
    gate_ref,
    up_ref,
    down_ref,
    gate2_ref,
    up2_ref,
    down2_ref,
    out_ref,
    taken,
    gate_w,
    up_w,
    down_w,
    product,
    back,
    token,
    own,
    arrive,
    leave,
    load_sem,
    weight_sem,
    near_send,
    near_recv,
    ring_send,
    ring_recv,
):
    z, c, ring, near = places()
    steps, taken_rows, width = taken.shape
    rows = out_ref.shape[0]
    part = width // SPLIT
    span = 2 * SLOTS
    group = steps // 2
    halves = ((group, steps), (0, group))
    loads = [
        pltpu.make_async_copy(
            sent_ref.at[pl.ds(a, b - a)], taken.at[pl.ds(a, b - a)], load_sem.at[i]
        )
        for i, (a, b) in enumerate(halves)
    ]
    weights = [
        pltpu.make_async_copy(source, target.at[i // 3], weight_sem.at[i])
        for i, (source, target) in enumerate(
            (
                (gate_ref, gate_w),
                (up_ref, up_w),
                (down_ref, down_w),
                (gate2_ref, gate_w),
                (up2_ref, up_w),
                (down2_ref, down_w),
            )
        )
    ]
    loads[0].start()
    for w in weights[:2]:
        w.start()
    loads[1].start()
    for w in weights[2:]:
        w.start()
    greet((*ring, *near))

    def near_copy(j, q):
        return pltpu.make_async_remote_copy(
            src_ref=product.at[j, pl.ds(q * span, span)],
            dst_ref=back.at[j, pl.ds(q * span, span)],
            send_sem=near_send.at[j, q - 1],
            recv_sem=near_recv.at[j, q - 1],
            device_id=near[q - 1],
            device_id_type=MESH,
        )

    def ring_copy(d, j, h):
        columns = pl.ds(h * part, part)
        slot = j - 1 if j > 0 else steps - 1
        return pltpu.make_async_remote_copy(
            src_ref=leave.at[d, j, :, columns],
            dst_ref=arrive.at[d, slot, :, columns],
            send_sem=ring_send.at[d, j, h],
            recv_sem=ring_recv.at[d, j, h],
            device_id=ring[1 - d],
            device_id_type=MESH,
        )

    for i, (a, b) in enumerate(halves):
        loads[i].wait()
        x = taken[a:b].reshape((b - a) * taken_rows, width)
        result = None
        for half in range(2):
            if i == 0:
                weights[3 * half].wait()
            gate = jnp.minimum(
                jnp.dot(x, gate_w[half], preferred_element_type=jnp.float32), limit
            )
            if i == 0:
                weights[3 * half + 1].wait()
            up = jnp.clip(
                jnp.dot(x, up_w[half], preferred_element_type=jnp.float32), -limit, limit
            )
            active = ((up + 1.0) * gate * jax.nn.sigmoid(slope * gate)).astype(jnp.bfloat16)
            if i == 0:
                weights[3 * half + 2].wait()
            term = jnp.dot(active, down_w[half], preferred_element_type=jnp.float32)
            result = term if result is None else result + term
        product[a:b] = result.astype(jnp.bfloat16).reshape(b - a, taken_rows, width)
        for j in range(b - 1, a - 1, -1):
            for q in (2, 3, 1):
                near_copy(j, q).start()
            back[j, 0:span] = product[j, 0:span]

    first = (steps - 1, steps - 2)
    for j in range(steps - 1, -1, -1):
        merged = notes_ref[j]
        found = matches(z, c, merged)
        tables = []
        for base in (4, 8):
            table = sum(
                jnp.where(m, jnp.broadcast_to(merged[base + k : base + k + 1], m.shape), 0.0)
                for k, m in enumerate(found)
            )
            flat = jnp.transpose(table)
            tables.append(jnp.concatenate([flat, flat], axis=1).astype(jnp.bfloat16))
        for q in (1, 2, 3):
            near_copy(j, q).wait_recv()
        token[...] = jnp.dot(tables[0], back[j], preferred_element_type=jnp.float32) + jnp.dot(
            tables[1], back[j], preferred_element_type=jnp.float32
        )
        if j == steps - 1:
            own[...] = token[HALF : HALF + rows]
        for h in range(SPLIT):
            columns = slice(h * part, (h + 1) * part)
            for d in range(2):
                if j > first[d]:
                    continue
                total = token[d * HALF : d * HALF + rows, columns]
                if j < first[d]:
                    ring_copy(d, j + 1, h).wait_recv()
                    total = total + arrive[d, j, :, columns].astype(jnp.float32)
                leave[d, j, :, columns] = total.astype(jnp.bfloat16)
                ring_copy(d, j, h).start()
    for h in range(SPLIT):
        columns = slice(h * part, (h + 1) * part)
        for d in range(2):
            ring_copy(d, 0, h).wait_recv()
        out_ref[:, columns] = (
            own[:, columns]
            + arrive[0, steps - 1, :, columns].astype(jnp.float32)
            + arrive[1, steps - 1, :, columns].astype(jnp.float32)
        )
    for j in range(steps):
        for q in (1, 2, 3):
            near_copy(j, q).wait_send()
        for d in range(2):
            if j <= first[d]:
                for h in range(SPLIT):
                    ring_copy(d, j, h).wait_send()


def combine(sent, notes, weights, rows):
    steps, taken_rows, width = sent.shape
    hidden_units = weights[0].shape[1]
    any_space = pl.BlockSpec(memory_space=pl.ANY)
    vmem = pl.BlockSpec(memory_space=pltpu.VMEM)
    bf16 = jnp.bfloat16
    return pl.pallas_call(
        combine_kernel,
        name="combine",
        out_shape=jax.ShapeDtypeStruct((rows, width), jnp.float32),
        in_specs=[any_space, vmem] + [any_space] * 6,
        out_specs=vmem,
        scratch_shapes=[
            pltpu.VMEM((steps, taken_rows, width), bf16),
            pltpu.VMEM((2, width, hidden_units), bf16),
            pltpu.VMEM((2, width, hidden_units), bf16),
            pltpu.VMEM((2, hidden_units, width), bf16),
            pltpu.VMEM((steps, taken_rows, width), bf16),
            pltpu.VMEM((steps, taken_rows, width), bf16),
            pltpu.VMEM((2 * HALF, width), jnp.float32),
            pltpu.VMEM((rows, width), jnp.float32),
            pltpu.VMEM((2, steps, rows, width), bf16),
            pltpu.VMEM((2, steps, rows, width), bf16),
            pltpu.SemaphoreType.DMA((2,)),
            pltpu.SemaphoreType.DMA((6,)),
            pltpu.SemaphoreType.DMA((steps, 3)),
            pltpu.SemaphoreType.DMA((steps, 3)),
            pltpu.SemaphoreType.DMA((2, steps, SPLIT)),
            pltpu.SemaphoreType.DMA((2, steps, SPLIT)),
        ],
        compiler_params=pltpu.CompilerParams(
            collective_id=2, has_side_effects=True, vmem_limit_bytes=56 * 2**20
        ),
        cost_estimate=pl.CostEstimate(
            flops=30_000_000_000, bytes_accessed=8_000_000, transcendentals=0
        ),
    )(sent, notes, *weights)


def attention_kernel(
    latent_ref,
    gain_ref,
    key_w_ref,
    value_w_ref,
    pairs_ref,
    query_ref,
    residual_ref,
    ffn_gain_ref,
    out_w_ref,
    hidden_ref,
    normed_ref,
    store,
    rots,
    summed,
    peaks,
    totals,
    staged,
    heads,
    out_w,
    out_w_sem,
    ring_send,
    ring_recv,
    rot_send,
    rot_recv,
    side_send,
    side_recv,
    side_rot_send,
    side_rot_recv,
    tp_send,
    tp_recv,
):
    z, c, ring, near = places()
    x = lax.axis_index("tp")
    tp = lax.axis_size("tp")
    steps = store.shape[0]
    tokens = latent_ref.shape[0]
    heads_dev = query_ref.shape[0]
    key_width = key_w_ref.shape[1]
    rows = residual_ref.shape[0]
    piece = tokens // SPLIT
    last = (steps - 1, steps - 2)
    load = pltpu.make_async_copy(out_w_ref, out_w, out_w_sem)
    load.start()
    wide = latent_ref[...].astype(jnp.float32)
    wide = (
        wide
        * lax.rsqrt(jnp.mean(wide * wide, axis=-1, keepdims=True) + eps)
        * gain_ref[...].astype(jnp.float32)
    ).astype(jnp.bfloat16)
    own = slice(2 * tokens, 3 * tokens)
    store[steps - 1, own, 0:key_width] = jnp.dot(
        wide, key_w_ref[...], preferred_element_type=jnp.float32
    ).astype(jnp.bfloat16)
    store[steps - 1, own, key_width:] = jnp.dot(
        wide, value_w_ref[...], preferred_element_type=jnp.float32
    ).astype(jnp.bfloat16)
    rots[steps - 1, 2] = pairs_ref[...]
    summed[...] = jnp.zeros_like(summed)
    totals[...] = jnp.zeros_like(totals)
    peaks[...] = jnp.full_like(peaks, -jnp.inf)
    others = [{"tp": lax.rem(x + r, tp)} for r in range(1, tp)]
    greet((*ring, near[0], *others))

    def ring_copy(d, j, h):
        source = (
            store.at[steps - 1, pl.ds(2 * tokens + h * piece, piece)]
            if j == 0
            else store.at[j - 1, pl.ds(2 * d * tokens + h * piece, piece)]
        )
        return pltpu.make_async_remote_copy(
            src_ref=source,
            dst_ref=store.at[j, pl.ds(2 * d * tokens + h * piece, piece)],
            send_sem=ring_send.at[d, j, h],
            recv_sem=ring_recv.at[d, j, h],
            device_id=ring[d],
            device_id_type=MESH,
        )

    def rot_copy(d, j):
        return pltpu.make_async_remote_copy(
            src_ref=pairs_ref if j == 0 else rots.at[j - 1, 2 * d],
            dst_ref=rots.at[j, 2 * d],
            send_sem=rot_send.at[d, j],
            recv_sem=rot_recv.at[d, j],
            device_id=ring[d],
            device_id_type=MESH,
        )

    def side_copy(d, j):
        return pltpu.make_async_remote_copy(
            src_ref=store.at[j, pl.ds(2 * d * tokens, tokens)],
            dst_ref=store.at[j, pl.ds((2 * d + 1) * tokens, tokens)],
            send_sem=side_send.at[d, j],
            recv_sem=side_recv.at[d, j],
            device_id=near[0],
            device_id_type=MESH,
        )

    def side_rot_copy(d, j):
        return pltpu.make_async_remote_copy(
            src_ref=rots.at[j, 2 * d],
            dst_ref=rots.at[j, 2 * d + 1],
            send_sem=side_rot_send.at[d, j],
            recv_sem=side_rot_recv.at[d, j],
            device_id=near[0],
            device_id_type=MESH,
        )

    def tp_copy(r):
        return pltpu.make_async_remote_copy(
            src_ref=staged.at[lax.rem(x + r, tp)],
            dst_ref=heads.at[x],
            send_sem=tp_send.at[r - 1],
            recv_sem=tp_recv.at[r - 1],
            device_id=others[r - 1],
            device_id_type=MESH,
        )

    factor = (PLAIN_HEAD_WIDTH + QK_ROPE) ** (-0.5) * 1.4426950408889634

    def attend(j):
        for d in range(2):
            side_copy(d, j).wait_recv()
            side_rot_copy(d, j).wait_recv()
        turned = []
        for b in range(4):
            pair = rots[j, b]
            turned.append(pair)
            turned.append(jnp.concatenate([pair[:, QK_ROPE:], pair[:, :QK_ROPE]], axis=1))
        turned = jnp.concatenate(turned, axis=0)
        for head in range(heads_dev):
            at = head * PLAIN_HEAD_WIDTH
            keys = jnp.concatenate([store[j, :, at : at + PLAIN_HEAD_WIDTH], turned], axis=1)
            scores = lax.dot_general(
                query_ref[head],
                keys,
                (((1,), (1,)), ((), ())),
                preferred_element_type=jnp.float32,
            )
            before = peaks[head]
            peak = jnp.maximum(before, jnp.max(scores, axis=1, keepdims=True))
            weights = jnp.exp2((scores - peak[:, 0:1]) * factor)
            keep = jnp.exp2((before - peak) * factor)
            totals[head] = totals[head] * keep + jnp.sum(weights, axis=1, keepdims=True)
            at = key_width + head * VALUE_WIDTH
            summed[head] = summed[head] * keep + jnp.dot(
                weights.astype(jnp.bfloat16),
                store[j, :, at : at + VALUE_WIDTH],
                preferred_element_type=jnp.float32,
            )
            peaks[head] = peak

    for h in range(SPLIT):
        for d in range(2):
            ring_copy(d, 0, h).start()
            if h == 0:
                rot_copy(d, 0).start()
    side_copy(1, steps - 1).start()
    side_rot_copy(1, steps - 1).start()
    for j in range(steps):
        for h in range(SPLIT):
            for d in range(2):
                if j <= last[d]:
                    ring_copy(d, j, h).wait_recv()
                    if j < last[d]:
                        ring_copy(d, j + 1, h).start()
                    if h == 0:
                        rot_copy(d, j).wait_recv()
                        if j < last[d]:
                            rot_copy(d, j + 1).start()
        for d in range(2):
            if j <= last[d]:
                side_copy(d, j).start()
                side_rot_copy(d, j).start()
        if j > 0:
            attend(j - 1)
    attend(steps - 1)
    done = jnp.concatenate(
        [summed[head] / totals[head] for head in range(heads_dev)], axis=1
    )
    for t in range(tp):
        staged[t] = done[t * rows : (t + 1) * rows].astype(jnp.bfloat16)
    for r in range(1, tp):
        tp_copy(r).start()
    heads[x] = staged[x]
    load.wait()
    for r in range(1, tp):
        tp_copy(r).wait_recv()
    total = residual_ref[...].astype(jnp.float32)
    width = heads.shape[2]
    for t in range(tp):
        total = total + jnp.dot(
            heads[t], out_w[t * width : (t + 1) * width], preferred_element_type=jnp.float32
        )
    hidden = total.astype(jnp.bfloat16)
    hidden_ref[...] = hidden
    wide = hidden.astype(jnp.float32)
    normed_ref[...] = (
        wide
        * lax.rsqrt(jnp.mean(wide * wide, axis=-1, keepdims=True) + eps)
        * ffn_gain_ref[...].astype(jnp.float32)
    ).astype(jnp.bfloat16)
    for r in range(1, tp):
        tp_copy(r).wait_send()
    for j in range(steps):
        for d in range(2):
            if j <= last[d]:
                rot_copy(d, j).wait_send()
                for h in range(SPLIT):
                    ring_copy(d, j, h).wait_send()
            side_copy(d, j).wait_send()
            side_rot_copy(d, j).wait_send()


def attention(
    latent, gain, key_w, value_w, pairs, query, residual, ffn_gain, out_w, steps, tp
):
    tokens = latent.shape[0]
    rows, width = residual.shape
    heads_dev = query.shape[0]
    store_width = key_w.shape[1] + value_w.shape[1]
    vmem = pl.BlockSpec(memory_space=pltpu.VMEM)
    bf16 = jnp.bfloat16
    dma = pltpu.SemaphoreType.DMA
    return pl.pallas_call(
        attention_kernel,
        name="attention",
        out_shape=(
            jax.ShapeDtypeStruct((rows, width), bf16),
            jax.ShapeDtypeStruct((rows, width), bf16),
        ),
        in_specs=[vmem] * 8 + [pl.BlockSpec(memory_space=pl.ANY)],
        out_specs=(vmem, vmem),
        scratch_shapes=[
            pltpu.VMEM((steps, 4 * tokens, store_width), bf16),
            pltpu.VMEM((steps, 4, *pairs.shape), bf16),
            pltpu.VMEM((heads_dev, tokens, VALUE_WIDTH), jnp.float32),
            pltpu.VMEM((heads_dev, tokens, VALUE_WIDTH), jnp.float32),
            pltpu.VMEM((heads_dev, tokens, VALUE_WIDTH), jnp.float32),
            pltpu.VMEM((tp, rows, heads_dev * VALUE_WIDTH), bf16),
            pltpu.VMEM((tp, rows, heads_dev * VALUE_WIDTH), bf16),
            pltpu.VMEM(out_w.shape, bf16),
            dma,
            dma((2, steps, SPLIT)),
            dma((2, steps, SPLIT)),
            dma((2, steps)),
            dma((2, steps)),
            dma((2, steps)),
            dma((2, steps)),
            dma((2, steps)),
            dma((2, steps)),
            dma((tp - 1,)),
            dma((tp - 1,)),
        ],
        compiler_params=pltpu.CompilerParams(
            collective_id=3, has_side_effects=True, vmem_limit_bytes=40 * 2**20
        ),
        cost_estimate=pl.CostEstimate(
            flops=30_000_000_000, bytes_accessed=8_000_000, transcendentals=0
        ),
    )(latent, gain, key_w, value_w, pairs, query, residual, ffn_gain, out_w)


def routing_note(routes, route_weights, experts):
    rows, top = routes.shape
    flat = routes.reshape(rows * top)
    marks = (flat[:, None] == jnp.arange(experts, dtype=jnp.int32)[None, :]).astype(jnp.int32)
    earlier = jnp.cumsum(marks, axis=0, dtype=jnp.int32) - marks
    slots = jnp.sum(earlier * marks, axis=1, dtype=jnp.int32)
    target = (flat * SLOTS + slots).reshape(rows, top)
    high = route_weights.astype(jnp.bfloat16)
    low = (route_weights - high.astype(jnp.float32)).astype(jnp.bfloat16)
    parts = jnp.concatenate([target.astype(jnp.bfloat16), high, low], axis=1).T
    return jnp.pad(
        parts, ((0, 16 - 3 * top), (0, 2 * HALF - rows)), constant_values=-1.0
    )


def on_device(
    query_plain,
    query_turn,
    latent,
    key_turn,
    latent_norm_scale,
    plain_key_matrix,
    value_matrix,
    residual,
    out_weight,
    ffn_gain,
    gate_weight,
    up_weight,
    down_weight,
    routes,
    route_weights,
):
    tok_dev = latent.shape[0]
    heads_dev = query_plain.shape[1] // PLAIN_HEAD_WIDTH
    tp = lax.axis_size("tp")
    swap = [(i, i ^ 1) for i in range(tp)]
    own_weights = (gate_weight[0], up_weight[0], down_weight[0])
    other_weights = tuple(lax.ppermute(w, "tp", swap) for w in own_weights)
    experts_all = lax.axis_size(SP) * gate_weight.shape[0]
    note = routing_note(routes, route_weights, experts_all)
    place = lax.axis_index(SP) * tok_dev + jnp.arange(tok_dev, dtype=jnp.int32)
    grid_row = place // GRID_W
    grid_col = place % GRID_W
    key_rot = turn(key_turn.astype(jnp.float32), grid_row, grid_col).astype(jnp.bfloat16)
    key_pairs = jnp.concatenate([key_rot[: tok_dev // 2], key_rot[tok_dev // 2 :]], axis=1)
    query_rot = turn(
        query_turn.astype(jnp.float32).reshape(tok_dev, heads_dev, QK_ROPE), grid_row, grid_col
    ).astype(jnp.bfloat16)
    plain_query = query_plain.reshape(tok_dev, heads_dev, PLAIN_HEAD_WIDTH)
    query = jnp.concatenate(
        [plain_query, query_rot, jnp.zeros_like(query_rot)], axis=2
    ).transpose(1, 0, 2)
    rows_dev = residual.shape[0]
    steps = lax.axis_size("sp_0") // 2
    hidden, normed = attention(
        latent,
        latent_norm_scale[None],
        plain_key_matrix,
        value_matrix,
        key_pairs,
        query,
        residual,
        ffn_gain[None],
        out_weight,
        steps,
        tp,
    )
    sent, notes = dispatch(normed, note, steps)
    mixed = combine(sent, notes, (*own_weights, *other_weights), rows_dev)
    return (hidden.astype(jnp.float32) + mixed).astype(jnp.bfloat16)


def solution(mesh):
    torus = Mesh(
        mesh.devices.reshape(mesh.shape["grp"], mesh.shape["sp"] // 2, 2, mesh.shape["tp"]),
        ("grp", "sp_0", "sp_1", "tp"),
    )
    placed = (
        P(GRP_SP, "tp"),
        P(GRP_SP, "tp"),
        P(GRP_SP, None),
        P(GRP_SP, None),
        P(),
        P(None, "tp"),
        P(None, "tp"),
        P(GRP_SP_TP, None),
        P(),
        P(),
        P(SP, None, "tp"),
        P(SP, None, "tp"),
        P(SP, "tp", None),
        P(GRP_SP_TP, None),
        P(GRP_SP_TP, None),
    )
    return jax.shard_map(
        on_device, mesh=torus, in_specs=placed, out_specs=P(GRP_SP_TP, None), check_vma=False
    )
```

```python
import math

import jax
import jax.numpy as jnp
from jax import lax
from jax.experimental import pallas as pl
from jax.experimental.pallas import tpu as pltpu
from jax.sharding import Mesh
from jax.sharding import PartitionSpec as P

PLAIN_HEAD_WIDTH = 128
QK_ROPE = 64
VALUE_WIDTH = 128
GRID_W = 64
SP = ("sp_0", "sp_1")
GRP_SP = ("grp", "sp_0", "sp_1")
GRP_SP_TP = ("grp", "sp_0", "sp_1", "tp")
MESH = pl.DeviceIdType.MESH

theta = 10000.0
eps = 1e-06
limit = 7.0
slope = 1.702

SLOTS = 8
HALF = 64
SPLIT = 2
CHUNKS = 8


def matches(z, c, target):
    row = lax.broadcasted_iota(jnp.int32, (4 * SLOTS, 2 * HALF), 0)
    lane = lax.broadcasted_iota(jnp.int32, (4 * SLOTS, 2 * HALF), 1)
    core = jnp.where(row < 2 * SLOTS, c, 1 - c)
    wanted = ((2 * z + core) * SLOTS + row % SLOTS).astype(jnp.float32)
    same = (row // SLOTS) % 2 == lane // HALF
    return [
        jnp.logical_and(same, jnp.broadcast_to(target[k : k + 1], wanted.shape) == wanted)
        for k in range(4)
    ]


def layer_kernel(
    latent_hbm,
    gain_ref,
    key_w_hbm,
    value_w_hbm,
    key_turn_ref,
    query_hbm,
    query_turn_hbm,
    residual_hbm,
    ffn_gain_ref,
    routes_ref,
    route_weights_ref,
    out_w_hbm,
    gate_hbm,
    up_hbm,
    down_hbm,
    out_ref,
    latent_ref,
    key_w_ref,
    value_w_ref,
    query_ref,
    query_turn_ref,
    residual_ref,
    out_w,
    query,
    store,
    rots,
    summed,
    peaks,
    totals,
    staged,
    heads,
    hidden_ref,
    notes,
    padded,
    blocks,
    chosen,
    taken,
    gate_w,
    up_w,
    down_w,
    product,
    back,
    token,
    own_part,
    arrive,
    leave,
    load_sem,
    weight_sem,
    chunk_send,
    chunk_recv,
    key_send,
    key_recv,
    rot_send,
    rot_recv,
    side_send,
    side_recv,
    side_rot_send,
    side_rot_recv,
    note_send,
    note_recv,
    tp_send,
    tp_recv,
    row_send,
    row_recv,
    go_send,
    go_recv,
    come_send,
    come_recv,
    sum_send,
    sum_recv,
):
    z = lax.axis_index("sp_0")
    c = lax.axis_index("sp_1")
    x = lax.axis_index("tp")
    tp = lax.axis_size("tp")
    ring_size = lax.axis_size("sp_0")
    mirror = tp - 1 - x
    mate = x + 1 - 2 * lax.rem(x, 2)
    ring = ({"sp_0": lax.rem(z + 1, ring_size)}, {"sp_0": lax.rem(z + ring_size - 1, ring_size)})
    near = ({"sp_1": 1 - c}, {"tp": mirror}, {"sp_1": 1 - c, "tp": mirror})
    others = [{"tp": lax.rem(x + r, tp)} for r in range(1, tp)]
    steps = store.shape[0]
    end = steps - 1
    tokens = latent_ref.shape[0]
    rows, width = residual_ref.shape
    heads_dev = query.shape[0]
    key_width = key_w_ref.shape[1]
    span = 2 * SLOTS

    loads = [
        pltpu.make_async_copy(source, target, load_sem.at[i])
        for i, (source, target) in enumerate(
            (
                (latent_hbm, latent_ref),
                (key_w_hbm, key_w_ref),
                (value_w_hbm, value_w_ref),
                (query_turn_hbm, query_turn_ref),
                (query_hbm, query_ref),
                (residual_hbm, residual_ref),
                (out_w_hbm, out_w),
            )
        )
    ]
    for load in loads:
        load.start()
    own_weights = [
        pltpu.make_async_copy(source.at[0], target.at[0], weight_sem.at[i])
        for i, (source, target) in enumerate(
            ((gate_hbm, gate_w), (up_hbm, up_w), (down_hbm, down_w))
        )
    ]
    for load in own_weights:
        load.start()

    barrier = pltpu.get_barrier_semaphore()
    greeted = (*ring, near[0], near[2], *others)
    for peer in greeted:
        pl.semaphore_signal(barrier, inc=1, device_id=peer, device_id_type=MESH)

    def remote(source, target, send_sem, recv_sem, device):
        return pltpu.make_async_remote_copy(
            src_ref=source,
            dst_ref=target,
            send_sem=send_sem,
            recv_sem=recv_sem,
            device_id=device,
            device_id_type=MESH,
        )

    def chunk_copy(i):
        kind, at = i // CHUNKS, i % CHUNKS
        source, target = ((gate_hbm, gate_w), (up_hbm, up_w), (down_hbm, down_w))[kind]
        size = source.shape[1] // CHUNKS
        part = pl.ds(at * size, size)
        return remote(
            source.at[0, part],
            target.at[1, part],
            chunk_send.at[i],
            chunk_recv.at[i],
            {"tp": mate},
        )

    issued = []

    def issue_chunks(upto):
        while len(issued) < min(upto, 3 * CHUNKS):
            chunk_copy(len(issued)).start()
            issued.append(None)

    def active(d, j, h):
        return j < end or h * 2 // SPLIT == d

    for j in range(steps):
        for d in range(2):
            blocks[j, d * HALF + rows : (d + 1) * HALF] = jnp.zeros(
                (HALF - rows, width), blocks.dtype
            )
    summed[...] = jnp.zeros_like(summed)
    totals[...] = jnp.zeros_like(totals)
    peaks[...] = jnp.full_like(peaks, -jnp.inf)

    lane = lax.broadcasted_iota(jnp.int32, (tokens, 2 * QK_ROPE), 1)
    place = lax.broadcasted_iota(jnp.int32, (tokens, 2 * QK_ROPE), 0) + (2 * z + c) * tokens
    count = QK_ROPE // 4
    upper = lax.rem(lane // count, 2) == 1
    by_column = lax.rem(lane // (2 * count), 2) == 1
    spot = jnp.where(by_column, lax.rem(place, GRID_W), place // GRID_W).astype(jnp.float32)
    freqs = jnp.exp(lax.rem(lane, count).astype(jnp.float32) * (-math.log(theta) / count))
    angle = spot * freqs
    cosine = jnp.cos(angle)
    sine = jnp.sin(angle)
    sine = jnp.where(upper, sine, -sine)

    def turned(values):
        partner = jnp.where(
            upper, pltpu.roll(values, count, 1), pltpu.roll(values, 2 * QK_ROPE - count, 1)
        )
        return values * cosine + partner * sine

    flat = jnp.transpose(key_turn_ref[...].astype(jnp.float32))
    twice = turned(jnp.concatenate([flat, flat], axis=1))
    left = lane < QK_ROPE
    rots[end, 2] = jnp.where(
        left[: tokens // 2], twice[: tokens // 2], twice[tokens // 2 :]
    ).astype(jnp.bfloat16)

    padded[0] = jnp.full(padded.shape[1:], -1.0, jnp.float32)
    padded[1] = jnp.zeros(padded.shape[1:], jnp.float32)
    top = routes_ref.shape[0]
    padded[0, 0:top, 0:rows] = routes_ref[...].astype(jnp.float32)
    padded[1, 0:top, 0:rows] = route_weights_ref[...]
    experts = 2 * ring_size
    lanes = 2 * HALF
    numbers = lax.broadcasted_iota(jnp.int32, (experts, lanes), 0).astype(jnp.float32)
    marks = [
        (jnp.broadcast_to(padded[0, k : k + 1], numbers.shape) == numbers).astype(jnp.float32)
        for k in range(top)
    ]
    earlier = (
        lax.broadcasted_iota(jnp.int32, (lanes, lanes), 0)
        < lax.broadcasted_iota(jnp.int32, (lanes, lanes), 1)
    ).astype(jnp.bfloat16)
    counts = jnp.dot(
        sum(marks).astype(jnp.bfloat16), earlier, preferred_element_type=jnp.float32
    )
    for k in range(top):
        slot = jnp.sum(marks[k] * counts, axis=0, keepdims=True)
        notes[1, end, k : k + 1] = padded[0, k : k + 1] * SLOTS + slot
        notes[1, end, top + k : top + k + 1] = padded[1, k : k + 1]

    for load in loads[:3]:
        load.wait()
    wide = latent_ref[...].astype(jnp.float32)
    wide = (
        wide
        * lax.rsqrt(jnp.mean(wide * wide, axis=-1, keepdims=True) + eps)
        * gain_ref[...].astype(jnp.float32)
    ).astype(jnp.bfloat16)
    mine = slice(2 * tokens, 3 * tokens)
    store[end, mine, 0:key_width] = jnp.dot(
        wide, key_w_ref[...], preferred_element_type=jnp.float32
    ).astype(jnp.bfloat16)
    store[end, mine, key_width:] = jnp.dot(
        wide, value_w_ref[...], preferred_element_type=jnp.float32
    ).astype(jnp.bfloat16)
    pl.semaphore_wait(barrier, len(greeted))

    piece = tokens // SPLIT

    def key_copy(d, j, h):
        source_step, source_slot = (end, 2) if j == 0 else (j - 1, 2 * d)
        slot = 2 * d if j < end else 0
        return remote(
            store.at[source_step, pl.ds(source_slot * tokens + h * piece, piece)],
            store.at[j, pl.ds(slot * tokens + h * piece, piece)],
            key_send.at[d, j, h],
            key_recv.at[d, j, h],
            ring[d],
        )

    def rot_copy(d, j):
        return remote(
            rots.at[end, 2] if j == 0 else rots.at[j - 1, 2 * d],
            rots.at[j, 2 * d],
            rot_send.at[d, j],
            rot_recv.at[d, j],
            ring[d],
        )

    def note_copy(d, j):
        return remote(
            notes.at[1, end] if j == 0 else notes.at[d, j - 1],
            notes.at[d, j],
            note_send.at[d, j],
            note_recv.at[d, j],
            ring[d],
        )

    def side_copy(d, j):
        return remote(
            store.at[j, pl.ds(2 * d * tokens, tokens)],
            store.at[j, pl.ds((2 * d + 1) * tokens, tokens)],
            side_send.at[d, j],
            side_recv.at[d, j],
            near[0],
        )

    def side_rot_copy(d, j):
        return remote(
            rots.at[j, 2 * d],
            rots.at[j, 2 * d + 1],
            side_rot_send.at[d, j],
            side_rot_recv.at[d, j],
            near[0],
        )

    def tp_copy(r):
        return remote(
            staged.at[lax.rem(x + r, tp)],
            heads.at[x],
            tp_send.at[r - 1],
            tp_recv.at[r - 1],
            others[r - 1],
        )

    factor = (PLAIN_HEAD_WIDTH + QK_ROPE) ** (-0.5) * 1.4426950408889634

    def attend(j):
        for d in range(2):
            side_copy(d, j).wait_recv()
            side_rot_copy(d, j).wait_recv()
        pairs = []
        for b in range(4):
            pair = rots[j, b]
            pairs.append(pair)
            pairs.append(jnp.concatenate([pair[:, QK_ROPE:], pair[:, :QK_ROPE]], axis=1))
        pairs = jnp.concatenate(pairs, axis=0)
        for head in range(heads_dev):
            at = head * PLAIN_HEAD_WIDTH
            keys = jnp.concatenate([store[j, :, at : at + PLAIN_HEAD_WIDTH], pairs], axis=1)
            scores = lax.dot_general(
                query[head],
                keys,
                (((1,), (1,)), ((), ())),
                preferred_element_type=jnp.float32,
            )
            before = peaks[head]
            peak = jnp.maximum(before, jnp.max(scores, axis=1, keepdims=True))
            weights = jnp.exp2((scores - peak[:, 0:1]) * factor)
            keep = jnp.exp2((before - peak) * factor)
            totals[head] = totals[head] * keep + jnp.sum(weights, axis=1, keepdims=True)
            at = key_width + head * VALUE_WIDTH
            summed[head] = summed[head] * keep + jnp.dot(
                weights.astype(jnp.bfloat16),
                store[j, :, at : at + VALUE_WIDTH],
                preferred_element_type=jnp.float32,
            )
            peaks[head] = peak

    for h in range(SPLIT):
        for d in range(2):
            key_copy(d, 0, h).start()
            if h == 0:
                rot_copy(d, 0).start()
    side_copy(1, end).start()
    side_rot_copy(1, end).start()
    for d in range(2):
        note_copy(d, 0).start()
    issue_chunks(2)
    for load in loads[3:5]:
        load.wait()
    spun = turned(query_turn_ref[...].astype(jnp.float32))
    for head in range(heads_dev):
        query[head, :, 0:PLAIN_HEAD_WIDTH] = query_ref[
            :, head * PLAIN_HEAD_WIDTH : (head + 1) * PLAIN_HEAD_WIDTH
        ]
        here = spun if head == 0 else pltpu.roll(spun, 2 * QK_ROPE - head * QK_ROPE, 1)
        query[head, :, PLAIN_HEAD_WIDTH:] = jnp.where(left, here, 0.0).astype(jnp.bfloat16)
    for j in range(steps):
        for h in range(SPLIT):
            for d in range(2):
                if active(d, j, h):
                    key_copy(d, j, h).wait_recv()
                    if j < end and active(d, j + 1, h):
                        key_copy(d, j + 1, h).start()
                if h == 0 and j <= end - d:
                    rot_copy(d, j).wait_recv()
                    if j < end - d:
                        rot_copy(d, j + 1).start()
        for d in range(2):
            if j <= end - d:
                side_copy(d, j).start()
                side_rot_copy(d, j).start()
                note_copy(d, j).wait_recv()
                if j < end - d:
                    note_copy(d, j + 1).start()
        if j < end:
            issue_chunks(2 + (j + 1) * 3 // 2)
        if j > 0:
            attend(j - 1)
    attend(end)
    done = jnp.concatenate([summed[head] / totals[head] for head in range(heads_dev)], axis=1)
    for t in range(tp):
        staged[t] = done[t * rows : (t + 1) * rows].astype(jnp.bfloat16)
    for r in range(1, tp):
        tp_copy(r).start()
    heads[x] = staged[x]
    for load in loads[5:]:
        load.wait()
    for r in range(1, tp):
        tp_copy(r).wait_recv()
    total = residual_ref[...].astype(jnp.float32)
    head_width = heads.shape[2]
    for t in range(tp):
        total = total + jnp.dot(
            heads[t],
            out_w[t * head_width : (t + 1) * head_width],
            preferred_element_type=jnp.float32,
        )
    hidden = total.astype(jnp.bfloat16)
    hidden_ref[...] = hidden
    wide = hidden.astype(jnp.float32)
    blocks[end, HALF : HALF + rows] = (
        wide
        * lax.rsqrt(jnp.mean(wide * wide, axis=-1, keepdims=True) + eps)
        * ffn_gain_ref[...].astype(jnp.float32)
    ).astype(jnp.bfloat16)

    part = width // SPLIT

    def row_copy(d, j, h):
        columns = pl.ds(h * part, part)
        source_step, source_side = (end, 1) if j == 0 else (j - 1, d)
        side = d if j < end else 0
        return remote(
            blocks.at[source_step, pl.ds(source_side * HALF, rows), columns],
            blocks.at[j, pl.ds(side * HALF, rows), columns],
            row_send.at[d, j, h],
            row_recv.at[d, j, h],
            ring[d],
        )

    def go_copy(j, q):
        return remote(
            chosen.at[j, pl.ds((q % 2) * span, span)],
            taken.at[j, pl.ds(q * span, span)],
            go_send.at[j, q - 1],
            go_recv.at[j, q - 1],
            near[q - 1],
        )

    def come_copy(j, q):
        return remote(
            product.at[j, pl.ds(q * span, span)],
            back.at[j, pl.ds(q * span, span)],
            come_send.at[j, q - 1],
            come_recv.at[j, q - 1],
            near[q - 1],
        )

    def sum_copy(d, j, h):
        columns = pl.ds(h * part, part)
        return remote(
            leave.at[d, j, :, columns],
            arrive.at[d, j - 1 if j > 0 else end, :, columns],
            sum_send.at[d, j, h],
            sum_recv.at[d, j, h],
            ring[1 - d],
        )

    def merged(j):
        return jnp.concatenate([notes[0, j][:, :HALF], notes[1, j][:, :HALF]], axis=1)

    for h in range(SPLIT):
        for d in range(2):
            row_copy(d, 0, h).start()
    issue_chunks(15)
    for j in range(steps):
        for h in range(SPLIT):
            for d in range(2):
                if active(d, j, h):
                    row_copy(d, j, h).wait_recv()
                    if j < end and active(d, j + 1, h):
                        row_copy(d, j + 1, h).start()
        picks = sum(m.astype(jnp.float32) for m in matches(z, c, merged(j))).astype(jnp.bfloat16)
        kept = jnp.dot(picks, blocks[j], preferred_element_type=jnp.float32).astype(jnp.bfloat16)
        chosen[j] = kept
        for q in (2, 3, 1):
            go_copy(j, q).start()
        taken[j, 0:span] = kept[0:span]
        issue_chunks(15 + (j + 1) * 3 // 2)
    issue_chunks(3 * CHUNKS)

    group = steps // 2
    for i, (a, b) in enumerate(((group, steps), (0, group))):
        for j in range(a, b):
            for q in (1, 2, 3):
                go_copy(j, q).wait_recv()
        given = taken[a:b].reshape((b - a) * 4 * span, width)
        result = None
        for half in range(2):
            def ready(kind):
                if i == 0 and half == 0:
                    own_weights[kind].wait()
                elif i == 0:
                    for at in range(CHUNKS):
                        chunk_copy(kind * CHUNKS + at).wait_recv()

            ready(0)
            gate = jnp.minimum(
                jnp.dot(given, gate_w[half], preferred_element_type=jnp.float32), limit
            )
            ready(1)
            up = jnp.clip(
                jnp.dot(given, up_w[half], preferred_element_type=jnp.float32), -limit, limit
            )
            act = ((up + 1.0) * gate * jax.nn.sigmoid(slope * gate)).astype(jnp.bfloat16)
            ready(2)
            term = jnp.dot(act, down_w[half], preferred_element_type=jnp.float32)
            result = term if result is None else result + term
        product[a:b] = result.astype(jnp.bfloat16).reshape(b - a, 4 * span, width)
        for j in range(b - 1, a - 1, -1):
            for q in (2, 3, 1):
                come_copy(j, q).start()
            back[j, 0:span] = product[j, 0:span]

    for j in range(end, -1, -1):
        both = merged(j)
        found = matches(z, c, both)
        table = sum(
            jnp.where(m, jnp.broadcast_to(both[top + k : top + k + 1], m.shape), 0.0)
            for k, m in enumerate(found)
        )
        table = jnp.transpose(table)
        table = jnp.concatenate([table, table], axis=1)
        high = table.astype(jnp.bfloat16)
        low = (table - high.astype(jnp.float32)).astype(jnp.bfloat16)
        for q in (1, 2, 3):
            come_copy(j, q).wait_recv()
        token[...] = jnp.dot(high, back[j], preferred_element_type=jnp.float32) + jnp.dot(
            low, back[j], preferred_element_type=jnp.float32
        )
        if j == end:
            own_part[...] = token[HALF : HALF + rows]
        for h in range(SPLIT):
            columns = slice(h * part, (h + 1) * part)
            for d in range(2):
                if not active(d, j, h):
                    continue
                at = d * HALF if j < end else 0
                total = token[at : at + rows, columns]
                if j < end and active(d, j + 1, h):
                    sum_copy(d, j + 1, h).wait_recv()
                    total = total + arrive[d, j, :, columns].astype(jnp.float32)
                leave[d, j, :, columns] = total.astype(jnp.bfloat16)
                sum_copy(d, j, h).start()
    for h in range(SPLIT):
        columns = slice(h * part, (h + 1) * part)
        for d in range(2):
            sum_copy(d, 0, h).wait_recv()
        out_ref[:, columns] = (
            hidden_ref[:, columns].astype(jnp.float32)
            + own_part[:, columns]
            + arrive[0, end, :, columns].astype(jnp.float32)
            + arrive[1, end, :, columns].astype(jnp.float32)
        ).astype(jnp.bfloat16)

    for i in range(3 * CHUNKS):
        chunk_copy(i).wait_send()
    for r in range(1, tp):
        tp_copy(r).wait_send()
    for j in range(steps):
        for d in range(2):
            for h in range(SPLIT):
                if active(d, j, h):
                    key_copy(d, j, h).wait_send()
                    row_copy(d, j, h).wait_send()
                    sum_copy(d, j, h).wait_send()
            if j <= end - d:
                rot_copy(d, j).wait_send()
                note_copy(d, j).wait_send()
            side_copy(d, j).wait_send()
            side_rot_copy(d, j).wait_send()
        for q in (1, 2, 3):
            go_copy(j, q).wait_send()
            come_copy(j, q).wait_send()


def on_device(
    query_plain,
    query_turn,
    latent,
    key_turn,
    latent_norm_scale,
    plain_key_matrix,
    value_matrix,
    residual,
    out_weight,
    ffn_gain,
    gate_weight,
    up_weight,
    down_weight,
    routes,
    route_weights,
):
    tokens = latent.shape[0]
    rows, width = residual.shape
    heads_dev = query_plain.shape[1] // PLAIN_HEAD_WIDTH
    tp = lax.axis_size("tp")
    steps = lax.axis_size("sp_0") // 2
    store_width = plain_key_matrix.shape[1] + value_matrix.shape[1]
    head_width = heads_dev * VALUE_WIDTH
    gate_shape, down_shape = gate_weight.shape[1:], down_weight.shape[1:]
    bf16, f32 = jnp.bfloat16, jnp.float32
    vmem, anywhere = pltpu.VMEM, pl.ANY
    dma = pltpu.SemaphoreType.DMA
    operands = (
        (latent, anywhere),
        (latent_norm_scale.reshape(1, -1), vmem),
        (plain_key_matrix, anywhere),
        (value_matrix, anywhere),
        (key_turn.T, vmem),
        (query_plain, anywhere),
        (query_turn, anywhere),
        (residual, anywhere),
        (ffn_gain.reshape(1, -1), vmem),
        (routes.T, vmem),
        (route_weights.T, vmem),
        (out_weight, anywhere),
        (gate_weight, anywhere),
        (up_weight, anywhere),
        (down_weight, anywhere),
    )
    both_ways = dma((2, steps))
    pieces = dma((2, steps, SPLIT))
    return pl.pallas_call(
        layer_kernel,
        name="layer",
        out_shape=jax.ShapeDtypeStruct((rows, width), bf16),
        in_specs=[pl.BlockSpec(memory_space=space) for _, space in operands],
        out_specs=pl.BlockSpec(memory_space=vmem),
        scratch_shapes=[
            vmem(latent.shape, bf16),
            vmem(plain_key_matrix.shape, bf16),
            vmem(value_matrix.shape, bf16),
            vmem(query_plain.shape, bf16),
            vmem(query_turn.shape, bf16),
            vmem(residual.shape, bf16),
            vmem(out_weight.shape, bf16),
            vmem((heads_dev, tokens, PLAIN_HEAD_WIDTH + 2 * QK_ROPE), bf16),
            vmem((steps, 4 * tokens, store_width), bf16),
            vmem((steps, 4, tokens // 2, 2 * QK_ROPE), bf16),
            vmem((heads_dev, tokens, VALUE_WIDTH), f32),
            vmem((heads_dev, tokens, VALUE_WIDTH), f32),
            vmem((heads_dev, tokens, VALUE_WIDTH), f32),
            vmem((tp, rows, head_width), bf16),
            vmem((tp, rows, head_width), bf16),
            vmem((rows, width), bf16),
            vmem((2, steps, 8, 2 * HALF), f32),
            vmem((2, 8, 2 * HALF), f32),
            vmem((steps, 2 * HALF, width), bf16),
            vmem((steps, 4 * SLOTS, width), bf16),
            vmem((steps, 8 * SLOTS, width), bf16),
            vmem((2, *gate_shape), bf16),
            vmem((2, *gate_shape), bf16),
            vmem((2, *down_shape), bf16),
            vmem((steps, 8 * SLOTS, width), bf16),
            vmem((steps, 8 * SLOTS, width), bf16),
            vmem((2 * HALF, width), f32),
            vmem((rows, width), f32),
            vmem((2, steps, rows, width), bf16),
            vmem((2, steps, rows, width), bf16),
            dma((7,)),
            dma((3,)),
            dma((3 * CHUNKS,)),
            dma((3 * CHUNKS,)),
            pieces,
            pieces,
            both_ways,
            both_ways,
            both_ways,
            both_ways,
            both_ways,
            both_ways,
            both_ways,
            both_ways,
            dma((tp - 1,)),
            dma((tp - 1,)),
            pieces,
            pieces,
            dma((steps, 3)),
            dma((steps, 3)),
            dma((steps, 3)),
            dma((steps, 3)),
            pieces,
            pieces,
        ],
        compiler_params=pltpu.CompilerParams(
            collective_id=1, has_side_effects=True, vmem_limit_bytes=60 * 2**20
        ),
        cost_estimate=pl.CostEstimate(
            flops=30_000_000_000, bytes_accessed=20_000_000, transcendentals=0
        ),
    )(*(array for array, _ in operands))


def solution(mesh):
    torus = Mesh(
        mesh.devices.reshape(mesh.shape["grp"], mesh.shape["sp"] // 2, 2, mesh.shape["tp"]),
        ("grp", "sp_0", "sp_1", "tp"),
    )
    placed = (
        P(GRP_SP, "tp"),
        P(GRP_SP, "tp"),
        P(GRP_SP, None),
        P(GRP_SP, None),
        P(),
        P(None, "tp"),
        P(None, "tp"),
        P(GRP_SP_TP, None),
        P(),
        P(),
        P(SP, None, "tp"),
        P(SP, None, "tp"),
        P(SP, "tp", None),
        P(GRP_SP_TP, None),
        P(GRP_SP_TP, None),
    )
    return jax.shard_map(
        on_device, mesh=torus, in_specs=placed, out_specs=P(GRP_SP_TP, None), check_vma=False
    )
```

```python
import math

import jax
import jax.numpy as jnp
from jax import lax
from jax.experimental import pallas as pl
from jax.experimental.pallas import tpu as pltpu
from jax.sharding import Mesh
from jax.sharding import PartitionSpec as P

PLAIN_HEAD_WIDTH = 128
QK_ROPE = 64
VALUE_WIDTH = 128
GRID_W = 64
SP = ("sp_0", "sp_1")
GRP_SP = ("grp", "sp_0", "sp_1")
GRP_SP_TP = ("grp", "sp_0", "sp_1", "tp")
MESH = pl.DeviceIdType.MESH

theta = 10000.0
eps = 1e-06
limit = 7.0
slope = 1.702

SLOTS = 8
HALF = 64
KEY_SPLIT = 2
ROW_SPLIT = 4
CHUNKS = 4


def matches(z, c, target):
    row = lax.broadcasted_iota(jnp.int32, (4 * SLOTS, 2 * HALF), 0)
    lane = lax.broadcasted_iota(jnp.int32, (4 * SLOTS, 2 * HALF), 1)
    core = jnp.where(row < 2 * SLOTS, c, 1 - c)
    wanted = ((2 * z + core) * SLOTS + row % SLOTS).astype(jnp.float32)
    same = (row // SLOTS) % 2 == lane // HALF
    return [
        jnp.logical_and(same, jnp.broadcast_to(target[k : k + 1], wanted.shape) == wanted)
        for k in range(4)
    ]


def layer_kernel(
    latent_hbm,
    gain_ref,
    key_w_hbm,
    value_w_hbm,
    key_turn_ref,
    query_hbm,
    query_turn_hbm,
    residual_hbm,
    ffn_gain_ref,
    routes_ref,
    route_weights_ref,
    out_w_hbm,
    gate_hbm,
    up_hbm,
    down_hbm,
    out_ref,
    latent_ref,
    kv_w,
    query_ref,
    query_turn_ref,
    residual_ref,
    out_w,
    query,
    store,
    rots,
    summed,
    peaks,
    totals,
    staged,
    heads,
    staged_logs,
    logs,
    hidden_ref,
    notes,
    padded,
    blocks,
    chosen,
    taken,
    gate_w,
    up_w,
    down_w,
    product,
    back,
    token,
    own_part,
    arrive,
    leave,
    load_sem,
    weight_sem,
    chunk_send,
    chunk_recv,
    cross_send,
    cross_recv,
    pair_send,
    pair_recv,
    key_send,
    key_recv,
    rot_send,
    rot_recv,
    side_send,
    side_recv,
    side_rot_send,
    side_rot_recv,
    note_send,
    note_recv,
    tp_send,
    tp_recv,
    row_send,
    row_recv,
    go_send,
    go_recv,
    come_send,
    come_recv,
    sum_send,
    sum_recv,
):
    z = lax.axis_index("sp_0")
    c = lax.axis_index("sp_1")
    x = lax.axis_index("tp")
    tp = lax.axis_size("tp")
    ring_size = lax.axis_size("sp_0")
    mirror = tp - 1 - x
    mate = x + 1 - 2 * lax.rem(x, 2)
    ring = ({"sp_0": lax.rem(z + 1, ring_size)}, {"sp_0": lax.rem(z + ring_size - 1, ring_size)})
    near = ({"sp_1": 1 - c}, {"tp": mirror}, {"sp_1": 1 - c, "tp": mirror})
    others = [{"tp": lax.rem(x + r, tp)} for r in range(1, tp)]
    groups = lax.axis_size("grp")
    shared = groups % 2 == 0
    parity = lax.rem(lax.axis_index("grp"), 2)
    across = {"grp": lax.axis_index("grp") + 1 - 2 * parity}
    steps = store.shape[0]
    end = steps - 1
    tokens = query_ref.shape[1]
    half_tokens = latent_ref.shape[0]
    rows, width = residual_ref.shape
    heads_dev = query.shape[0]
    key_width = kv_w.shape[2] // 2
    span = 2 * SLOTS
    later = x // (tp // 2)

    loads = [
        pltpu.make_async_copy(source, target, load_sem.at[i])
        for i, (source, target) in enumerate(
            (
                (latent_hbm.at[pl.ds(later * half_tokens, half_tokens)], latent_ref),
                (key_w_hbm, kv_w.at[0, :, pl.ds(0, key_width)]),
                (value_w_hbm, kv_w.at[0, :, pl.ds(key_width, key_width)]),
                (query_turn_hbm, query_turn_ref.at[0]),
                (query_hbm, query_ref.at[0]),
                (residual_hbm, residual_ref),
                (out_w_hbm, out_w),
            )
        )
    ]
    for load in loads:
        load.start()
    own_weights = [
        pltpu.make_async_copy(source.at[0], target.at[0], weight_sem.at[i])
        for i, (source, target) in enumerate(
            ((gate_hbm, gate_w), (up_hbm, up_w), (down_hbm, down_w))
        )
    ]
    for load in own_weights:
        load.start()

    barrier = pltpu.get_barrier_semaphore()
    greeted = (*ring, near[0], near[2], *others, *((across,) if shared else ()))
    for peer in greeted:
        pl.semaphore_signal(barrier, inc=1, device_id=peer, device_id_type=MESH)

    def remote(source, target, send_sem, recv_sem, device):
        return pltpu.make_async_remote_copy(
            src_ref=source,
            dst_ref=target,
            send_sem=send_sem,
            recv_sem=recv_sem,
            device_id=device,
            device_id_type=MESH,
        )

    chunks = 3 * CHUNKS if shared else 6 * CHUNKS

    def chunk_parts(i):
        each = chunks // 3
        kind, at = i // each, i % each
        source, target = ((gate_hbm, gate_w), (up_hbm, up_w), (down_hbm, down_w))[kind]
        size = source.shape[1] // (2 * CHUNKS)
        first = parity * (CHUNKS * size) if shared else 0
        return source, target, pl.ds(pl.multiple_of(first + at * size, size), size)

    def chunk_copy(i):
        source, target, part = chunk_parts(i)
        return remote(
            source.at[0, part],
            target.at[1, part],
            chunk_send.at[i],
            chunk_recv.at[i],
            {"tp": mate},
        )

    def cross_copy(i):
        _, target, part = chunk_parts(i)
        return remote(
            target.at[1, part], target.at[1, part], cross_send.at[i], cross_recv.at[i], across
        )

    issued, crossed = [], []

    def issue_chunks(upto):
        while len(issued) < min(upto, chunks):
            chunk_copy(len(issued)).start()
            issued.append(None)

    def cross_chunks(upto):
        while shared and len(crossed) < min(upto, chunks):
            chunk_copy(len(crossed)).wait_recv()
            cross_copy(len(crossed)).start()
            crossed.append(None)

    def active(d, j, h, split):
        return j < end or h * 2 // split == d

    loads[0].wait()
    wide = latent_ref[...].astype(jnp.float32)
    mine = slice(half_tokens, 2 * half_tokens)
    store[end, mine] = (
        wide
        * lax.rsqrt(jnp.mean(wide * wide, axis=-1, keepdims=True) + eps)
        * gain_ref[...].astype(jnp.float32)
    ).astype(jnp.bfloat16)
    for load in loads[1:5]:
        load.wait()
    pl.semaphore_wait(barrier, len(greeted))

    latent_part = store.shape[2] // KEY_SPLIT
    depth = kv_w.shape[1] // 2

    def key_copy(d, j, h):
        source_step, source_slot = (end, 1) if j == 0 else (j - 1, d)
        slot = d if j < end else 0
        columns = pl.ds(h * latent_part, latent_part)
        return remote(
            store.at[source_step, pl.ds(source_slot * half_tokens, half_tokens), columns],
            store.at[j, pl.ds(slot * half_tokens, half_tokens), columns],
            key_send.at[d, j, h],
            key_recv.at[d, j, h],
            ring[d],
        )

    def rot_copy(d, j):
        return remote(
            rots.at[end, 1] if j == 0 else rots.at[j - 1, d],
            rots.at[j, d],
            rot_send.at[d, j],
            rot_recv.at[d, j],
            ring[d],
        )

    def note_copy(d, j):
        return remote(
            notes.at[1, end] if j == 0 else notes.at[d, j - 1],
            notes.at[d, j],
            note_send.at[d, j],
            note_recv.at[d, j],
            ring[d],
        )

    def side_copy(d, j):
        return remote(
            store.at[j, pl.ds(d * half_tokens, half_tokens)],
            store.at[j, pl.ds((2 + d) * half_tokens, half_tokens)],
            side_send.at[d, j],
            side_recv.at[d, j],
            near[0],
        )

    def side_rot_copy(d, j):
        return remote(
            rots.at[j, d],
            rots.at[j, 2 + d],
            side_rot_send.at[d, j],
            side_rot_recv.at[d, j],
            near[0],
        )

    core_rows = pl.ds(pl.multiple_of(c * depth, depth), depth)
    pair_copies = [
        remote(source, target, pair_send.at[i], pair_recv.at[i], near[1])
        for i, (source, target) in enumerate(
            (
                (query_turn_ref.at[0], query_turn_ref.at[1]),
                (query_ref.at[0], query_ref.at[1]),
                (kv_w.at[0, core_rows], kv_w.at[1, core_rows]),
            )
        )
    ]
    other_rows = pl.ds(pl.multiple_of((1 - c) * depth, depth), depth)
    pair_side = remote(
        kv_w.at[1, core_rows], kv_w.at[1, core_rows], pair_send.at[3], pair_recv.at[3], near[0]
    )

    def tp_copy(r, kind):
        source, target = ((staged, heads), (staged_logs, logs))[kind]
        return remote(
            source.at[lax.rem(x + r, tp)],
            target.at[x],
            tp_send.at[r - 1, kind],
            tp_recv.at[r - 1, kind],
            others[r - 1],
        )

    log2e = 1.4426950408889634
    factor = (PLAIN_HEAD_WIDTH + QK_ROPE) ** (-0.5) * log2e

    def attend(j, side):
        if side:
            for d in range(2):
                side_copy(d, j).wait_recv()
                side_rot_copy(d, j).wait_recv()
        at = slice(2 * side * half_tokens, 2 * (side + 1) * half_tokens)
        latents = store[j, at]
        spins = rots[j, 2 * side : 2 * side + 2].reshape(2 * half_tokens, 2 * QK_ROPE)
        for owner in range(2):
            both = jnp.dot(latents, kv_w[owner], preferred_element_type=jnp.float32).astype(
                jnp.bfloat16
            )
            for local in range(heads_dev // 2):
                head = owner * (heads_dev // 2) + local
                first = local * PLAIN_HEAD_WIDTH
                keys = jnp.concatenate([both[:, first : first + PLAIN_HEAD_WIDTH], spins], axis=1)
                scores = lax.dot_general(
                    query[head],
                    keys,
                    (((1,), (1,)), ((), ())),
                    preferred_element_type=jnp.float32,
                )
                before = peaks[head]
                peak = jnp.maximum(before, jnp.max(scores, axis=1, keepdims=True))
                weights = jnp.exp2((scores - peak[:, 0:1]) * factor)
                keep = jnp.exp2((before - peak) * factor)
                totals[head] = totals[head] * keep + jnp.sum(weights, axis=1, keepdims=True)
                first = key_width + local * VALUE_WIDTH
                summed[head] = summed[head] * keep + jnp.dot(
                    weights.astype(jnp.bfloat16),
                    both[:, first : first + VALUE_WIDTH],
                    preferred_element_type=jnp.float32,
                )
                peaks[head] = peak

    for h in range(KEY_SPLIT):
        for d in range(2):
            key_copy(d, 0, h).start()
    side_copy(1, end).start()
    for copy in pair_copies:
        copy.start()
    issue_chunks(3)

    lane = lax.broadcasted_iota(jnp.int32, (tokens, 2 * QK_ROPE), 1)
    place = lax.broadcasted_iota(jnp.int32, (tokens, 2 * QK_ROPE), 0) + (2 * z + c) * tokens
    count = QK_ROPE // 4
    upper = lax.rem(lane // count, 2) == 1
    by_column = lax.rem(lane // (2 * count), 2) == 1
    spot = jnp.where(by_column, lax.rem(place, GRID_W), place // GRID_W).astype(jnp.float32)
    freqs = jnp.exp(lax.rem(lane, count).astype(jnp.float32) * (-math.log(theta) / count))
    angle = spot * freqs
    cosine = jnp.cos(angle)
    sine = jnp.sin(angle)
    sine = jnp.where(upper, sine, -sine)

    def turned(values):
        partner = jnp.where(
            upper, pltpu.roll(values, count, 1), pltpu.roll(values, 2 * QK_ROPE - count, 1)
        )
        return values * cosine + partner * sine

    flat = jnp.transpose(key_turn_ref[...].astype(jnp.float32))
    twice = turned(jnp.concatenate([flat, flat], axis=1))
    left = lane < QK_ROPE
    rots[end, 1] = jnp.where(later == 0, twice[:half_tokens], twice[half_tokens:]).astype(
        jnp.bfloat16
    )
    for d in range(2):
        rot_copy(d, 0).start()
    side_rot_copy(1, end).start()
    padded[0] = jnp.full(padded.shape[1:], -1.0, jnp.float32)
    padded[1] = jnp.zeros(padded.shape[1:], jnp.float32)
    top = routes_ref.shape[0]
    padded[0, 0:top, 0:rows] = routes_ref[...].astype(jnp.float32)
    padded[1, 0:top, 0:rows] = route_weights_ref[...]
    experts = 2 * ring_size
    lanes = 2 * HALF
    numbers = lax.broadcasted_iota(jnp.int32, (experts, lanes), 0).astype(jnp.float32)
    marks = [
        (jnp.broadcast_to(padded[0, k : k + 1], numbers.shape) == numbers).astype(jnp.float32)
        for k in range(top)
    ]
    earlier = (
        lax.broadcasted_iota(jnp.int32, (lanes, lanes), 0)
        < lax.broadcasted_iota(jnp.int32, (lanes, lanes), 1)
    ).astype(jnp.bfloat16)
    counts = jnp.dot(
        sum(marks).astype(jnp.bfloat16), earlier, preferred_element_type=jnp.float32
    )
    for k in range(top):
        slot = jnp.sum(marks[k] * counts, axis=0, keepdims=True)
        notes[1, end, k : k + 1] = padded[0, k : k + 1] * SLOTS + slot
        notes[1, end, top + k : top + k + 1] = padded[1, k : k + 1]

    for d in range(2):
        note_copy(d, 0).start()
    summed[...] = jnp.zeros_like(summed)
    totals[...] = jnp.zeros_like(totals)
    peaks[...] = jnp.full_like(peaks, -jnp.inf)

    def place_queries(owner):
        spun = turned(query_turn_ref[owner].astype(jnp.float32))
        for local in range(heads_dev // 2):
            head = owner * (heads_dev // 2) + local
            query[head, :, 0:PLAIN_HEAD_WIDTH] = query_ref[
                owner, :, local * PLAIN_HEAD_WIDTH : (local + 1) * PLAIN_HEAD_WIDTH
            ]
            here = spun if local == 0 else pltpu.roll(spun, 2 * QK_ROPE - local * QK_ROPE, 1)
            query[head, :, PLAIN_HEAD_WIDTH:] = jnp.where(left, here, 0.0).astype(jnp.bfloat16)

    place_queries(0)
    plan = [[] for _ in range(steps)]
    plan[1] = [(0, 0), (0, 1)]
    plan[2] = [(1, 0), (1, 1), (2, 0)]
    for j in range(3, steps):
        plan[j] = [(j - 1, 1), (j, 0)]
    for j in range(steps):
        for h in range(KEY_SPLIT):
            for d in range(2):
                if active(d, j, h, KEY_SPLIT):
                    key_copy(d, j, h).wait_recv()
                    if j < end and active(d, j + 1, h, KEY_SPLIT):
                        key_copy(d, j + 1, h).start()
        for d in range(2):
            if j <= end - d:
                side_copy(d, j).start()
                rot_copy(d, j).wait_recv()
                if j < end - d:
                    rot_copy(d, j + 1).start()
                side_rot_copy(d, j).start()
                note_copy(d, j).wait_recv()
                if j < end - d:
                    note_copy(d, j + 1).start()
        if j < end:
            issue_chunks(4 + j)
        if j == 0:
            for p in range(steps):
                for d in range(2):
                    blocks[p, d * HALF + rows : (d + 1) * HALF] = jnp.zeros(
                        (HALF - rows, width), blocks.dtype
                    )
        if j == 1:
            pair_copies[2].wait_recv()
            pair_side.start()
            for copy in pair_copies[:2]:
                copy.wait_recv()
            place_queries(1)
            pair_side_in = remote(
                kv_w.at[1, other_rows], kv_w.at[1, other_rows], pair_send.at[3], pair_recv.at[3], near[0]
            )
            pair_side_in.wait_recv()
        for unit in plan[j]:
            attend(*unit)
        cross_chunks(j - 1)
    attend(end, 1)
    logs_all = jnp.zeros((tokens, 2 * QK_ROPE), jnp.float32)
    done = []
    for head in range(heads_dev):
        total = totals[head]
        done.append(summed[head] / total)
        logs_all = jnp.where(
            lane == head, peaks[head] * factor + jnp.log(total) * log2e, logs_all
        )
    done = jnp.concatenate(done, axis=1)
    for t in range(tp):
        staged[t] = done[t * rows : (t + 1) * rows].astype(jnp.bfloat16)
        staged_logs[t] = logs_all[t * rows : (t + 1) * rows]
    for r in range(1, tp):
        for kind in range(2):
            tp_copy(r, kind).start()
    heads[x] = staged[x]
    logs[x] = staged_logs[x]
    for load in loads[5:]:
        load.wait()
    for r in range(1, tp):
        for kind in range(2):
            tp_copy(r, kind).wait_recv()
    total = residual_ref[...].astype(jnp.float32)
    for t in range(tp):
        joined = []
        for local in range(heads_dev // 2):
            alone = []
            for owner, source in enumerate((t, tp - 1 - t)):
                head = owner * (heads_dev // 2) + local
                part = heads[source, :, head * VALUE_WIDTH : (head + 1) * VALUE_WIDTH]
                alone.append((part.astype(jnp.float32), logs[source][:, head : head + 1]))
            (a, log_a), (b, log_b) = alone
            top_log = jnp.maximum(log_a, log_b)
            share_a, share_b = jnp.exp2(log_a - top_log), jnp.exp2(log_b - top_log)
            joined.append((a * share_a + b * share_b) / (share_a + share_b))
        joined = jnp.concatenate(joined, axis=1).astype(jnp.bfloat16)
        head_width = joined.shape[1]
        total = total + jnp.dot(
            joined,
            out_w[t * head_width : (t + 1) * head_width],
            preferred_element_type=jnp.float32,
        )
    hidden = total.astype(jnp.bfloat16)
    hidden_ref[...] = hidden
    wide = hidden.astype(jnp.float32)
    blocks[end, HALF : HALF + rows] = (
        wide
        * lax.rsqrt(jnp.mean(wide * wide, axis=-1, keepdims=True) + eps)
        * ffn_gain_ref[...].astype(jnp.float32)
    ).astype(jnp.bfloat16)

    part = width // ROW_SPLIT

    def row_copy(d, j, h):
        columns = pl.ds(h * part, part)
        source_step, source_side = (end, 1) if j == 0 else (j - 1, d)
        side = d if j < end else 0
        return remote(
            blocks.at[source_step, pl.ds(source_side * HALF, rows), columns],
            blocks.at[j, pl.ds(side * HALF, rows), columns],
            row_send.at[d, j, h],
            row_recv.at[d, j, h],
            ring[d],
        )

    def go_copy(j, q):
        return remote(
            chosen.at[j, pl.ds((q % 2) * span, span)],
            taken.at[j, pl.ds(q * span, span)],
            go_send.at[j, q - 1],
            go_recv.at[j, q - 1],
            near[q - 1],
        )

    def come_copy(j, q):
        return remote(
            product.at[j, pl.ds(q * span, span)],
            back.at[j, pl.ds(q * span, span)],
            come_send.at[j, q - 1],
            come_recv.at[j, q - 1],
            near[q - 1],
        )

    def sum_copy(d, j, h):
        columns = pl.ds(h * part, part)
        return remote(
            leave.at[d, j, :, columns],
            arrive.at[d, j - 1 if j > 0 else end, :, columns],
            sum_send.at[d, j, h],
            sum_recv.at[d, j, h],
            ring[1 - d],
        )

    def merged(j):
        return jnp.concatenate([notes[0, j][:, :HALF], notes[1, j][:, :HALF]], axis=1)

    for h in range(ROW_SPLIT):
        for d in range(2):
            row_copy(d, 0, h).start()
    issue_chunks(chunks if shared else chunks // 2)
    for j in range(steps):
        for h in range(ROW_SPLIT):
            for d in range(2):
                if active(d, j, h, ROW_SPLIT):
                    row_copy(d, j, h).wait_recv()
                    if j < end and active(d, j + 1, h, ROW_SPLIT):
                        row_copy(d, j + 1, h).start()
        picks = sum(m.astype(jnp.float32) for m in matches(z, c, merged(j))).astype(jnp.bfloat16)
        kept = jnp.dot(picks, blocks[j], preferred_element_type=jnp.float32).astype(jnp.bfloat16)
        chosen[j] = kept
        for q in (2, 3, 1):
            go_copy(j, q).start()
        taken[j, 0:span] = kept[0:span]
        issue_chunks(chunks // 2 + 2 * (j + 1))
        cross_chunks(end - 1 + j)
    issue_chunks(chunks)
    cross_chunks(chunks)

    group = steps // 2
    for i, (a, b) in enumerate(((group, steps), (0, group))):
        for j in range(a, b):
            for q in (1, 2, 3):
                go_copy(j, q).wait_recv()
        given = taken[a:b].reshape((b - a) * 4 * span, width)
        result = None
        for half in range(2):
            def ready(kind):
                if i == 0 and half == 0:
                    own_weights[kind].wait()
                elif i == 0:
                    for at in range(kind * chunks // 3, (kind + 1) * chunks // 3):
                        (cross_copy if shared else chunk_copy)(at).wait_recv()

            ready(0)
            gate = jnp.minimum(
                jnp.dot(given, gate_w[half], preferred_element_type=jnp.float32), limit
            )
            ready(1)
            up = jnp.clip(
                jnp.dot(given, up_w[half], preferred_element_type=jnp.float32), -limit, limit
            )
            act = ((up + 1.0) * gate * jax.nn.sigmoid(slope * gate)).astype(jnp.bfloat16)
            ready(2)
            term = jnp.dot(act, down_w[half], preferred_element_type=jnp.float32)
            result = term if result is None else result + term
        product[a:b] = result.astype(jnp.bfloat16).reshape(b - a, 4 * span, width)
        for j in range(b - 1, a - 1, -1):
            for q in (2, 3, 1):
                come_copy(j, q).start()
            back[j, 0:span] = product[j, 0:span]

    for j in range(end, -1, -1):
        both = merged(j)
        found = matches(z, c, both)
        table = sum(
            jnp.where(m, jnp.broadcast_to(both[top + k : top + k + 1], m.shape), 0.0)
            for k, m in enumerate(found)
        )
        table = jnp.transpose(table)
        table = jnp.concatenate([table, table], axis=1)
        high = table.astype(jnp.bfloat16)
        low = (table - high.astype(jnp.float32)).astype(jnp.bfloat16)
        for q in (1, 2, 3):
            come_copy(j, q).wait_recv()
        token[...] = jnp.dot(high, back[j], preferred_element_type=jnp.float32) + jnp.dot(
            low, back[j], preferred_element_type=jnp.float32
        )
        if j == end:
            own_part[...] = token[HALF : HALF + rows]
        for h in range(ROW_SPLIT):
            columns = slice(h * part, (h + 1) * part)
            for d in range(2):
                if not active(d, j, h, ROW_SPLIT):
                    continue
                at = d * HALF if j < end else 0
                total = token[at : at + rows, columns]
                if j < end and active(d, j + 1, h, ROW_SPLIT):
                    sum_copy(d, j + 1, h).wait_recv()
                    total = total + arrive[d, j, :, columns].astype(jnp.float32)
                leave[d, j, :, columns] = total.astype(jnp.bfloat16)
                sum_copy(d, j, h).start()
    for h in range(ROW_SPLIT):
        columns = slice(h * part, (h + 1) * part)
        for d in range(2):
            sum_copy(d, 0, h).wait_recv()
        out_ref[:, columns] = (
            hidden_ref[:, columns].astype(jnp.float32)
            + own_part[:, columns]
            + arrive[0, end, :, columns].astype(jnp.float32)
            + arrive[1, end, :, columns].astype(jnp.float32)
        ).astype(jnp.bfloat16)

    for i in range(chunks):
        chunk_copy(i).wait_send()
        if shared:
            cross_copy(i).wait_send()
    for copy in (*pair_copies, pair_side):
        copy.wait_send()
    for r in range(1, tp):
        for kind in range(2):
            tp_copy(r, kind).wait_send()
    for j in range(steps):
        for d in range(2):
            for h in range(KEY_SPLIT):
                if active(d, j, h, KEY_SPLIT):
                    key_copy(d, j, h).wait_send()
            for h in range(ROW_SPLIT):
                if active(d, j, h, ROW_SPLIT):
                    row_copy(d, j, h).wait_send()
                    sum_copy(d, j, h).wait_send()
            if j <= end - d:
                rot_copy(d, j).wait_send()
                note_copy(d, j).wait_send()
            side_copy(d, j).wait_send()
            side_rot_copy(d, j).wait_send()
        for q in (1, 2, 3):
            go_copy(j, q).wait_send()
            come_copy(j, q).wait_send()


def on_device(
    query_plain,
    query_turn,
    latent,
    key_turn,
    latent_norm_scale,
    plain_key_matrix,
    value_matrix,
    residual,
    out_weight,
    ffn_gain,
    gate_weight,
    up_weight,
    down_weight,
    routes,
    route_weights,
):
    tokens, latent_width = latent.shape
    half_tokens = tokens // 2
    rows, width = residual.shape
    heads_dev = 2 * query_plain.shape[1] // PLAIN_HEAD_WIDTH
    tp = lax.axis_size("tp")
    steps = lax.axis_size("sp_0") // 2
    store_width = plain_key_matrix.shape[1] + value_matrix.shape[1]
    head_width = heads_dev * VALUE_WIDTH
    gate_shape, down_shape = gate_weight.shape[1:], down_weight.shape[1:]
    bf16, f32 = jnp.bfloat16, jnp.float32
    vmem, anywhere = pltpu.VMEM, pl.ANY
    dma = pltpu.SemaphoreType.DMA
    operands = (
        (latent, anywhere),
        (latent_norm_scale.reshape(1, -1), vmem),
        (plain_key_matrix, anywhere),
        (value_matrix, anywhere),
        (key_turn.T, vmem),
        (query_plain, anywhere),
        (query_turn, anywhere),
        (residual, anywhere),
        (ffn_gain.reshape(1, -1), vmem),
        (routes.T, vmem),
        (route_weights.T, vmem),
        (out_weight, anywhere),
        (gate_weight, anywhere),
        (up_weight, anywhere),
        (down_weight, anywhere),
    )
    both_ways = dma((2, steps))
    pieces = dma((2, steps, ROW_SPLIT))
    return pl.pallas_call(
        layer_kernel,
        name="layer",
        out_shape=jax.ShapeDtypeStruct((rows, width), bf16),
        in_specs=[pl.BlockSpec(memory_space=space) for _, space in operands],
        out_specs=pl.BlockSpec(memory_space=vmem),
        scratch_shapes=[
            vmem((half_tokens, latent_width), bf16),
            vmem((2, latent_width, store_width), bf16),
            vmem((2, *query_plain.shape), bf16),
            vmem((2, *query_turn.shape), bf16),
            vmem(residual.shape, bf16),
            vmem(out_weight.shape, bf16),
            vmem((heads_dev, tokens, PLAIN_HEAD_WIDTH + 2 * QK_ROPE), bf16),
            vmem((steps, 4 * half_tokens, latent_width), bf16),
            vmem((steps, 4, half_tokens, 2 * QK_ROPE), bf16),
            vmem((heads_dev, tokens, VALUE_WIDTH), f32),
            vmem((heads_dev, tokens, VALUE_WIDTH), f32),
            vmem((heads_dev, tokens, VALUE_WIDTH), f32),
            vmem((tp, rows, head_width), bf16),
            vmem((tp, rows, head_width), bf16),
            vmem((tp, rows, 2 * QK_ROPE), f32),
            vmem((tp, rows, 2 * QK_ROPE), f32),
            vmem((rows, width), bf16),
            vmem((2, steps, 8, 2 * HALF), f32),
            vmem((2, 8, 2 * HALF), f32),
            vmem((steps, 2 * HALF, width), bf16),
            vmem((steps, 4 * SLOTS, width), bf16),
            vmem((steps, 8 * SLOTS, width), bf16),
            vmem((2, *gate_shape), bf16),
            vmem((2, *gate_shape), bf16),
            vmem((2, *down_shape), bf16),
            vmem((steps, 8 * SLOTS, width), bf16),
            vmem((steps, 8 * SLOTS, width), bf16),
            vmem((2 * HALF, width), f32),
            vmem((rows, width), f32),
            vmem((2, steps, rows, width), bf16),
            vmem((2, steps, rows, width), bf16),
            dma((7,)),
            dma((3,)),
            dma((6 * CHUNKS,)),
            dma((6 * CHUNKS,)),
            dma((3 * CHUNKS,)),
            dma((3 * CHUNKS,)),
            dma((4,)),
            dma((4,)),
            dma((2, steps, KEY_SPLIT)),
            dma((2, steps, KEY_SPLIT)),
            both_ways,
            both_ways,
            both_ways,
            both_ways,
            both_ways,
            both_ways,
            both_ways,
            both_ways,
            dma((tp - 1, 2)),
            dma((tp - 1, 2)),
            pieces,
            pieces,
            dma((steps, 3)),
            dma((steps, 3)),
            dma((steps, 3)),
            dma((steps, 3)),
            pieces,
            pieces,
        ],
        compiler_params=pltpu.CompilerParams(
            collective_id=1, has_side_effects=True, vmem_limit_bytes=60 * 2**20
        ),
        cost_estimate=pl.CostEstimate(
            flops=30_000_000_000, bytes_accessed=20_000_000, transcendentals=0
        ),
    )(*(array for array, _ in operands))


def solution(mesh):
    torus = Mesh(
        mesh.devices.reshape(mesh.shape["grp"], mesh.shape["sp"] // 2, 2, mesh.shape["tp"]),
        ("grp", "sp_0", "sp_1", "tp"),
    )
    placed = (
        P(GRP_SP, "tp"),
        P(GRP_SP, "tp"),
        P(GRP_SP, None),
        P(GRP_SP, None),
        P(),
        P(None, "tp"),
        P(None, "tp"),
        P(GRP_SP_TP, None),
        P(),
        P(),
        P(SP, None, "tp"),
        P(SP, None, "tp"),
        P(SP, "tp", None),
        P(GRP_SP_TP, None),
        P(GRP_SP_TP, None),
    )
    return jax.shard_map(
        on_device, mesh=torus, in_specs=placed, out_specs=P(GRP_SP_TP, None), check_vma=False
    )
```
